32 devices in a mesh: fs: 8 (over z, y), tp: 4 (over x, core).
Axes of the slice: x: 2, y: 2, z: 4, core: 2. Of those that a mesh axis runs over, the one named last changes fastest.
Arguments:
- tokens: bfloat16 [4096, 2048], P('fs'), may hold values from -6 to 6
- norm_gain: float32 [2048], P('fs'), may hold values from 0.1 to 1.9
- gate_weight: float32 [2048, 6144], P('fs', 'tp'), may hold values from -0.125 to 0.125
- up_weight: float32 [2048, 6144], P('fs', 'tp'), may hold values from -0.125 to 0.125
- down_weight: float32 [6144, 2048], P('fs', 'tp'), may hold values from -0.109375 to 0.109375
Outputs:
- mixed: bfloat16 [4096, 2048], P('fs', 'tp')
- gate_out: bfloat16 [2048, 6144], P(None, 'tp')
- up_out: bfloat16 [2048, 6144], P(None, 'tp')
- down_out: bfloat16 [6144, 2048], P('tp')
The draws below stay inside these ranges and needn't reach their ends.
All inputs are finite; a program needn't handle non-finite values.
Results may differ from the reference program's by a relative error of at most 0.014.
Values may be sent and summed in bfloat16 or wider, within the bound.
A program may use at most 128 MiB of HBM per device.

```python
import jax
import jax.numpy as jnp
from jax import lax

D = 2048
FF = 6144
TOKENS = 4096
N_TP = 4


def strengthened(drawn, stream_key, source, target, blocks, factor):
    def block_of(position):
        return (jnp.arange(drawn.shape[position]) // (drawn.shape[position] // blocks)).reshape((-1,) + (1,) * (drawn.ndim - 1 - position))

    first = jax.random.permutation(stream_key, blocks)[block_of(target)]
    other_side = (block_of(target) + blocks // 2) % blocks
    return jnp.where((block_of(source) == first) | (block_of(source) == other_side), factor * drawn, drawn)


def block_levels(rng, shape, shards, least, largest):
    gain, own = 1.0, jax.random.fold_in(rng, 6)
    for position, shards_of in shards:
        heights = jnp.exp(jax.random.uniform(jax.random.fold_in(own, position), (shards_of,), jnp.float32, least / len(shards), largest / len(shards)))
        gain = gain * jnp.repeat(heights, shape[position] // shards_of).reshape([-1 if axis == position else 1 for axis in range(len(shape))])
    return gain


def noise(own_key, extent, scale, reach, pieces=(), kind=jnp.bfloat16):
    values = jax.random.normal(own_key, extent, jnp.float32) * scale
    if len(pieces) > 0:
        values = block_levels(own_key, extent, pieces, -0.22, 0.18) * values
    return jnp.clip(values, min=-reach, max=reach).astype(kind)


def bell_draw_with(rng, dims, scale, bound, cuts, heavy, held_as=jnp.bfloat16):
    array = scale * jax.random.normal(rng, dims, jnp.float32)
    if cuts:
        array = array * block_levels(rng, dims, cuts, -0.22, 0.18)
    return jnp.clip(strengthened(array, jax.random.fold_in(rng, 3), *heavy), -bound, bound).astype(held_as)


def setup_inputs(seed: int = 0) -> dict:
    key_list = jax.random.split(jax.random.key(seed), 6)
    return {
        "tokens": noise(key_list[0], (TOKENS, D), 1.0, 6.0, ((0, 8),)),
        "norm_gain": jnp.clip(1.0 + 0.18 * jax.random.normal(key_list[1], (D,), jnp.float32), 0.1, 1.9),
        "gate_weight": noise(key_list[2], (D, FF), D ** -0.5, 0.125, ((0, 8), (1, 4)), jnp.float32),
        "up_weight": noise(key_list[3], (D, FF), D ** -0.5, 0.125, ((0, 8), (1, 4)), jnp.float32),
        "down_weight": bell_draw_with(key_list[4], (FF, D), FF ** -0.5, 0.109375, ((0, 8), (1, 4)), (0, 1, 8, 2.0), jnp.float32),
    }


def reference(tokens, norm_gain, gate_weight, up_weight, down_weight):
    gate_out = (norm_gain[:, None] * gate_weight).astype(jnp.bfloat16)
    up_out = (norm_gain[:, None] * up_weight).astype(jnp.bfloat16)
    down_out = down_weight.astype(jnp.bfloat16)
    values = tokens.astype(jnp.float32)
    normed = (values * jax.lax.rsqrt(lax.optimization_barrier(jnp.mean(values * values, axis=1, keepdims=True)) + 1e-05)).astype(jnp.bfloat16)
    gate = jnp.dot(normed, gate_out, preferred_element_type=jnp.float32)
    up = jnp.dot(normed, up_out, preferred_element_type=jnp.float32)
    hidden = (jax.nn.silu(gate) * up).astype(jnp.bfloat16)
    width = FF // N_TP
    total = jnp.zeros((tokens.shape[0], D), jnp.float32)
    for block in range(N_TP):
        part = jnp.dot(hidden[:, block * width:(block + 1) * width], down_out[block * width:(block + 1) * width, :], preferred_element_type=jnp.float32)
        total = total + part.astype(jnp.bfloat16).astype(jnp.float32)
    mixed = total.astype(jnp.bfloat16)
    return (mixed, gate_out, up_out, down_out)
```

```python
import functools

import jax
import jax.numpy as jnp
from jax import lax
from jax.experimental import pallas as pl
from jax.experimental.pallas import tpu as pltpu
from jax.sharding import PartitionSpec as P

MESH = pl.DeviceIdType.MESH
GRANT = 26 * 1024 * 1024
W = 128
LAG = 4
ORDER = (5, 0, 2, 6, 1, 3, 4, 7)


def lines(fs):
    y = 1
    while 2 * (2 * y) * (2 * y) <= fs:
        y *= 2
    return fs // y, y


def when(cond, fn):
    pl.when(cond)(fn)


def each(lo, hi, fn):
    if hi > lo:
        pl.loop(lo, hi)(fn)


def layer_kernel(
    Z, Y, T, nk, paired,
    gain_hbm, g_hbm, u_hbm, d_hbm, x_hbm,
    wg, wu, wd, mixed,
    gain_row, stage_g, stage_u, stage_d, own_d, transit, normed, hidden, part, near, pair, far,
    in_gain, in_g, in_u, in_d, in_x, s_up, s_dn, s_y, s_det, r_w, s_one, s_tz, s_tx, r_t,
    s_dz, s_dy, r_d, s_a, r_a, s_b, r_b,
):
    f, t = lax.axis_index("fs"), lax.axis_index("tp")
    X = T // 2
    z, y = f // Y, lax.rem(f, Y)
    x, core = t // 2, lax.rem(t, 2)
    has_up, has_dn = z < Z - 1, z > 0
    up, dn = (f + Y, t), (f - Y, t)
    others = [lax.rem(y + i, Y) for i in range(1, Y)]
    across = [(z * Y + o, t) for o in others]
    rows = g_hbm.shape[0]
    ck = rows // nk
    rows_d, cols_d = d_hbm.shape
    pq = cols_d // W
    nc = T * pq
    n = x_hbm.shape[0]
    staged, full = (stage_g, stage_u), (wg, wu)
    pieces = [(k, a) for k in range(nk) for a in range(2)]

    def load(k, a):
        at = pl.ds(k * ck, ck)
        return pltpu.make_async_copy((g_hbm, u_hbm)[a].at[at, :], staged[a].at[at, :], (in_g, in_u)[a].at[k])

    load_d = pltpu.make_async_copy(d_hbm, stage_d, in_d.at[0])
    load_x = pltpu.make_async_copy(x_hbm, normed, in_x.at[0])
    load_gain = pltpu.make_async_copy(gain_hbm, gain_row, in_gain.at[0])
    load_gain.start()
    for k, a in pieces:
        load(k, a).start()
    load_d.start()
    load_x.start()

    barrier = pltpu.get_barrier_semaphore()

    def greet(dev):
        pl.semaphore_signal(barrier, inc=1, device_id=dev, device_id_type=MESH)

    when(has_up, lambda: greet(up))
    when(has_dn, lambda: greet(dn))
    for dev in across:
        greet(dev)
    for i in range(1, T):
        greet((f, lax.rem(t + i, T)))

    load_gain.wait()
    diagonal = lax.broadcasted_iota(jnp.int32, (rows, rows), 0) == lax.broadcasted_iota(jnp.int32, (rows, rows), 1)
    gain = jnp.sum(jnp.where(diagonal, jnp.broadcast_to(gain_row[...], (rows, rows)), 0.0), axis=1, keepdims=True)

    def copy(src, dst, ss, rs, dev):
        return pltpu.make_async_remote_copy(
            src_ref=src, dst_ref=dst, send_sem=ss, recv_sem=rs, device_id=dev, device_id_type=MESH
        )

    def weight(a, k, source, ss, dev):
        at = full[a].at[pl.ds(pl.multiple_of(source * rows + k * ck, ck), ck), :]
        return copy(at, at, ss, r_w.at[source, a, k], dev)

    def arrived(a, k, source):
        weight(a, k, source, s_det.at[a, k], (f, lax.rem(t + 1, T))).wait_recv()

    sent = []

    def start(cond, make):
        sent.append((cond, make))
        if cond is None:
            make().start()
        else:
            when(cond, lambda: make().start())

    def scale(k, a):
        load(k, a).wait()
        at = pl.ds(pl.multiple_of(f * rows + k * ck, ck), ck)
        full[a][at, :] = (gain[k * ck:(k + 1) * ck, :] * staged[a][pl.ds(k * ck, ck), :]).astype(jnp.bfloat16)

    def send_own(k, a):
        start(has_up, lambda: weight(a, k, f, s_up.at[z, a, k], up))
        start(has_dn, lambda: weight(a, k, f, s_dn.at[z, a, k], dn))
        for i in range(Y - 1):
            start(None, lambda i=i: weight(a, k, f, s_y.at[i, z, a, k], across[i]))

    scale(*pieces[0])
    scale(*pieces[1])
    pl.semaphore_wait(barrier, Y + T - 2 + has_up.astype(jnp.int32) + has_dn.astype(jnp.int32))
    for i, piece in enumerate(pieces):
        if i + 2 < len(pieces):
            scale(*pieces[i + 2])
        send_own(*piece)

    def cols(j):
        return pl.ds(pl.multiple_of(j * W, W), W)

    def line_rows(line):
        return pl.ds(pl.multiple_of(line * rows_d, rows_d), rows_d)

    def down(line, j, ss, dev):
        at = wd.at[line_rows(line), cols(j)]
        return copy(at, at, ss, r_d.at[line, j], dev)

    def down_arrived(line, j):
        down(line, j, s_dy.at[0, j], (f, lax.rem(t + 1, T))).wait_recv()

    load_d.wait()
    own_d[...] = stage_d[...].astype(jnp.bfloat16)

    @pl.when(z == t)
    def _():
        wd[line_rows(y), pl.ds(pl.multiple_of(t * cols_d, cols_d), cols_d)] = stage_d[...].astype(jnp.bfloat16)

    def first(p):
        return copy(
            own_d.at[:, pl.ds(p * W, W)], wd.at[line_rows(y), cols(t * pq + p)],
            s_one.at[p], r_d.at[y, t * pq + p], (f, z),
        )

    load_x.wait()
    slab = 64 if n % 64 == 0 else n

    def normalise(i):
        at = pl.ds(pl.multiple_of(i * slab, slab), slab)
        v = normed[at, :].astype(jnp.float32)
        normed[at, :] = (v * lax.rsqrt(jnp.mean(v * v, axis=1, keepdims=True) + 1e-05)).astype(jnp.bfloat16)

    normalise(0)
    for p in range(pq):
        start(z != t, lambda p=p: first(p))
    each(1, n // slab, normalise)

    at_home = z == t
    can_up = jnp.logical_and(has_up, z >= t)
    can_dn = jnp.logical_and(has_dn, z <= t)
    inner = jnp.logical_and(has_up, has_dn)
    if paired:
        half = t // (T // 2)
        shift = (nc // 2) * (1 - half)
        far_up, far_dn = half == 0, half == 1
        beyond = jnp.logical_or(jnp.logical_and(z < t, far_dn), jnp.logical_and(z > t, far_up))
        fwd_mid = jnp.logical_or(
            jnp.logical_and(can_up, jnp.logical_not(far_up)), jnp.logical_and(can_dn, jnp.logical_not(far_dn))
        )
        mid_lo, mid_hi = 2 * pq, 2 * pq + pq // 2
    else:
        shift = 0
        mid_lo, mid_hi = 0, nc
    fwd_all = jnp.logical_or(can_up, can_dn)
    away = jnp.logical_not(at_home)

    def column(r):
        return lax.rem(r + shift, nc)

    bent = (pq if paired else 0, lambda i: column(core * pq + i))
    low = (pq if paired else 0, lambda i: column((1 - core) * pq + i))
    mid = (mid_hi - mid_lo, lambda i: column(mid_lo + i))
    high = (nc - mid_hi, lambda i: column(mid_hi + i))

    def over(kind, fn):
        each(0, kind[0], lambda i: fn(kind[1](i)))

    def both(a, b):
        return jnp.logical_and(a, b)

    def z_send(line, j, which, direction):
        return down(line, j, s_dz.at[direction, which, j], (up, dn)[direction])

    def near_ok(direction):
        return jnp.logical_not((far_up, far_dn)[direction])

    def can(direction):
        return (can_up, can_dn)[direction]

    def cross(j):
        for i in range(Y - 1):
            down(y, j, s_dy.at[i, j], across[i]).start()

    other = others[0]

    def assemble():
        for i in range(1, T):
            owner = lax.rem(t + i, T)
            for p in range(pq):
                down_arrived(y, owner * pq + p)
        over(high, cross)
        if paired:
            @pl.when(inner)
            def _():
                over(low, cross)
                over(mid, cross)

    if paired:
        guest = lax.rem(t + T // 2, T)
        guest_dn = guest // (T // 2) == 1
        guest_here = jnp.logical_or(both(z < guest, guest_dn), both(z > guest, jnp.logical_not(guest_dn)))
        guest_on = (both(both(z >= guest, has_up), jnp.logical_not(guest_dn)), both(both(z <= guest, has_dn), guest_dn))

        def relay(p, direction, src):
            return copy(
                src.at[:, cols(p)], transit.at[:, cols(p)], s_tz.at[p], r_t.at[p], (up, dn)[direction]
            )

        def hand_over(p):
            return copy(
                transit.at[:, cols(p)], wd.at[line_rows(y), cols(t * pq + p)], s_tx.at[p], r_d.at[y, t * pq + p], (f, guest)
            )

    def leave(direction):
        if paired:
            @pl.when(both(z == guest, guest_on[direction]))
            def _():
                each(0, pq, lambda p: relay(p, direction, own_d).start())

        @pl.when(both(at_home, can(direction)))
        def _():
            if paired:
                @pl.when(near_ok(direction))
                def _():
                    over(bent, lambda j: z_send(y, j, 0, direction).start())
            for kind in (low, mid, high):
                over(kind, lambda j: z_send(y, j, 0, direction).start())

    def hook(s):
        when(z == s, lambda: leave(0))
        when(z == Z - 1 - s, lambda: leave(1))

    for step in range(1, Z):
        for count, (k, a) in enumerate(pieces):
            if step == 1 and count == len(pieces) // 2:
                when(at_home, assemble)
            for sign in (-1, 1):
                zs = z + sign * step
                source = zs * Y + y
                valid = zs >= 0 if sign < 0 else zs < Z
                onward = jnp.logical_and(valid, has_up if sign < 0 else has_dn)
                when(valid, lambda a=a, k=k, s=source: arrived(a, k, s))
                if sign < 0:
                    start(onward, lambda a=a, k=k, s=source, q=zs: weight(a, k, s, s_up.at[q, a, k], up))
                else:
                    start(onward, lambda a=a, k=k, s=source, q=zs: weight(a, k, s, s_dn.at[q, a, k], dn))
                crossing = valid
                if paired and step == 1:
                    crossing = both(valid, zs != (0 if sign < 0 else Z - 1))
                for i in range(Y - 1):
                    start(crossing, lambda a=a, k=k, s=source, q=zs, i=i: weight(a, k, s, s_y.at[i, q, a, k], across[i]))
        if step == 1:
            hook(0)
            if paired:
                ends = jnp.logical_not(inner)
                beside = across[0][0]
                for k, a in pieces:
                    when(ends, lambda a=a, k=k: arrived(a, k, beside))
                    start(both(ends, has_up), lambda a=a, k=k: weight(a, k, beside, s_det.at[a, k], up))
                    start(both(ends, has_dn), lambda a=a, k=k: weight(a, k, beside, s_det.at[a, k], dn))
        hook(step)

    if paired:
        @pl.when(at_home)
        def _():
            @pl.when(jnp.logical_not(inner))
            def _():
                over(low, cross)
                over(mid, cross)
            over(bent, cross)

    else:
        when(at_home, lambda: over(mid, cross))

    if paired:
        @pl.when(guest_here)
        def _():
            def pass_on(p):
                copy(
                    transit.at[:, cols(p)], transit.at[:, cols(p)], s_tz.at[p], r_t.at[p], (f, guest)
                ).wait_recv()
                for direction in range(2):
                    when(guest_on[direction], lambda: relay(p, direction, transit).start())
                hand_over(p).start()
            each(0, pq, pass_on)

    @pl.when(away)
    def _():
        def bend(j):
            down_arrived(y, j)
            for direction in range(2):
                when(both(can(direction), near_ok(direction)), lambda: z_send(y, j, 0, direction).start())
            cross(j)

        def straight(j):
            down_arrived(y, j)
            for direction in range(2):
                when(can(direction), lambda: z_send(y, j, 0, direction).start())
            if paired:
                when(beyond, lambda: cross(j))
            else:
                cross(j)

        over(bent, bend)
        over(low, straight)
        over(mid, straight)

    if paired:
        @pl.when(fwd_mid)
        def _():
            def twin(j):
                down_arrived(other, j)
                for direction in range(2):
                    when(both(can(direction), near_ok(direction)), lambda: z_send(other, j, 1, direction).start())
            over(low, twin)
            over(mid, twin)

        @pl.when(fwd_all)
        def _():
            def twins(j):
                @pl.when(away)
                def _():
                    down_arrived(y, j)
                    for direction in range(2):
                        when(can(direction), lambda: z_send(y, j, 0, direction).start())
                down_arrived(other, j)
                for direction in range(2):
                    when(can(direction), lambda: z_send(other, j, 1, direction).start())
            over(high, twins)

    for zs in range(Z):
        for o in others:
            for k, a in pieces:
                if paired and zs in (0, Z - 1):
                    when(zs != z, lambda a=a, k=k, zs=zs, o=o: arrived(a, k, zs * Y + o))
                else:
                    arrived(a, k, zs * Y + o)
    units = wg.shape[1]
    width = 256 if units % 256 == 0 else 128

    @pl.loop(0, units // width)
    def _(j):
        at = pl.ds(pl.multiple_of(j * width, width), width)
        gate = jnp.dot(normed[...], wg[:, at], preferred_element_type=jnp.float32)
        up_ = jnp.dot(normed[...], wu[:, at], preferred_element_type=jnp.float32)
        hidden[:, at] = (gate / (1.0 + jnp.exp(-gate)) * up_).astype(jnp.bfloat16)

    for cond, make in sent:
        if cond is None:
            make().wait_send()
        else:
            when(cond, lambda make=make: make().wait_send())

    mate = (f, x * 2 + 1 - core)

    def piece_of(i):
        if not paired:
            return i
        eighth = sum(g * (i // (nc // 8) == e).astype(jnp.int32) for e, g in enumerate(ORDER))
        r = eighth * (nc // 8) + lax.rem(i, nc // 8)
        return lax.rem(r + (nc // 2) * (z >= Z // 2).astype(jnp.int32), nc)

    def to_mate(j):
        return copy(part.at[:, cols(j)], near.at[:, cols(j)], s_a.at[j], r_a.at[j], mate)

    def to_owner(j):
        owner = j // pq
        slot = lax.rem(x - owner // 2 + X, X) - 1
        p = lax.rem(j, pq)
        return copy(pair.at[:, cols(j)], far.at[slot, :, cols(p)], s_b.at[j], r_b.at[slot, p], (f, owner))

    def product(i):
        j = piece_of(i)
        if paired:
            r = lax.rem(j - shift + nc, nc)
            is_high = r >= mid_hi
            is_bent = both(r < 2 * pq, r // pq == core)
            is_mid = jnp.logical_not(jnp.logical_or(is_high, is_bent))
            late = both(is_high, jnp.logical_not(fwd_all))
            when(both(late, away), lambda: down_arrived(y, j))
            late_other = jnp.logical_or(jnp.logical_or(late, is_bent), both(is_mid, jnp.logical_not(fwd_mid)))
            when(late_other, lambda: down_arrived(other, j))
        else:
            for o in others:
                down_arrived(o, j)
        part[:, cols(j)] = jnp.dot(hidden[...], wd[:, cols(j)], preferred_element_type=jnp.float32).astype(jnp.bfloat16)

    def ours(j):
        return lax.rem(j // pq, 2) == core

    def at_owner_chip(j):
        return j // pq // 2 == x

    @pl.loop(0, nc + LAG)
    def _(i):
        now = i < nc
        last = both(i >= 1, i <= nc)
        done = i >= LAG
        j0 = piece_of(jnp.minimum(i, nc - 1))
        j1 = piece_of(jnp.minimum(jnp.maximum(i - 1, 0), nc - 1))
        j2 = piece_of(jnp.maximum(i - LAG, 0))
        when(now, lambda: product(i))
        mine = both(last, ours(j1))
        ship = both(mine, jnp.logical_not(at_owner_chip(j1)))
        when(mine, lambda: to_mate(j1).wait_recv())

        @pl.when(ship)
        def _():
            pair[:, cols(j1)] = (
                part[:, cols(j1)].astype(jnp.float32) + near[:, cols(j1)].astype(jnp.float32)
            ).astype(jnp.bfloat16)

        when(both(now, jnp.logical_not(ours(j0))), lambda: to_mate(j0).start())

        @pl.when(both(done, j2 // pq == t))
        def _():
            p = lax.rem(j2, pq)
            acc = part[:, cols(j2)].astype(jnp.float32) + near[:, cols(j2)].astype(jnp.float32)
            for slot in range(X - 1):
                copy(
                    pair.at[:, cols(j2)], far.at[slot, :, cols(p)], s_b.at[j2], r_b.at[slot, p], mate
                ).wait_recv()
                acc = acc + far[slot, :, cols(p)].astype(jnp.float32)
            mixed[:, cols(p)] = acc.astype(mixed.dtype)

        when(ship, lambda: to_owner(j1).start())

    if paired:
        def relayed(p):
            for direction in range(2):
                when(guest_on[direction], lambda: relay(p, direction, transit).wait_send())
            when(guest_here, lambda: hand_over(p).wait_send())
        each(0, pq, relayed)

    def crossed(j):
        for i in range(Y - 1):
            down(y, j, s_dy.at[i, j], across[i]).wait_send()

    def left(line, which, allowed):
        def fn(j):
            for direction in range(2):
                when(allowed(direction), lambda: z_send(line, j, which, direction).wait_send())
        return fn

    if paired:
        over(bent, left(y, 0, lambda d: both(can(d), near_ok(d))))
        for kind in (low, mid):
            over(kind, left(other, 1, lambda d: both(can(d), near_ok(d))))
        over(high, left(other, 1, can))
        over(bent, crossed)
        for kind in (low, mid):
            when(jnp.logical_or(at_home, beyond), lambda kind=kind: over(kind, crossed))
        when(at_home, lambda: over(high, crossed))
    else:
        over(mid, crossed)
    for kind in (low, mid, high):
        over(kind, left(y, 0, can))

    def swept(j):
        when(jnp.logical_not(ours(j)), lambda: to_mate(j).wait_send())
        when(both(ours(j), jnp.logical_not(at_owner_chip(j))), lambda: to_owner(j).wait_send())
    each(0, nc, swept)


def layer(mesh, gain, g, u, d, x):
    fs, T = mesh.shape["fs"], mesh.shape["tp"]
    Z, Y = lines(fs)
    X = T // 2
    rows, rows_d, n = g.shape[0], d.shape[0], x.shape[0]
    pq = d.shape[1] // W
    nc = T * pq
    nk = max(1, min(4, rows // 64))
    paired = Y == 2 and X == 2 and Z == T and pq % 2 == 0
    lanes = max(Y - 1, 1)
    dma = pltpu.SemaphoreType.DMA
    vmem, hbm = pl.BlockSpec(memory_space=pltpu.VMEM), pl.BlockSpec(memory_space=pltpu.HBM)
    bf = jnp.bfloat16
    return pl.pallas_call(
        functools.partial(layer_kernel, Z, Y, T, nk, paired),
        out_shape=(
            jax.ShapeDtypeStruct((rows * fs, g.shape[1]), bf),
            jax.ShapeDtypeStruct((rows * fs, g.shape[1]), bf),
            jax.ShapeDtypeStruct((rows_d * Y, d.shape[1] * T), bf),
            jax.ShapeDtypeStruct((n, d.shape[1]), bf),
        ),
        in_specs=[hbm] * 5,
        out_specs=[vmem] * 4,
        scratch_shapes=[
            pltpu.VMEM(gain.shape, jnp.float32),
            pltpu.VMEM(g.shape, jnp.float32), pltpu.VMEM(u.shape, jnp.float32), pltpu.VMEM(d.shape, jnp.float32),
            pltpu.VMEM(d.shape, bf), pltpu.VMEM(d.shape, bf), pltpu.VMEM(x.shape, bf), pltpu.VMEM((n, g.shape[1]), bf),
            pltpu.VMEM((n, nc * W), bf), pltpu.VMEM((n, nc * W), bf), pltpu.VMEM((n, nc * W), bf),
            pltpu.VMEM((max(X - 1, 1), n, pq * W), bf),
            dma((1,)), dma((nk,)), dma((nk,)), dma((1,)), dma((1,)),
            dma((Z, 2, nk)), dma((Z, 2, nk)), dma((lanes, Z, 2, nk)), dma((2, nk)), dma((fs, 2, nk)),
            dma((pq,)), dma((pq,)), dma((pq,)), dma((pq,)),
            dma((2, 2, nc)), dma((lanes, nc)), dma((Y, nc)),
            dma((nc,)), dma((nc,)), dma((nc,)), dma((max(X - 1, 1), pq)),
        ],
        compiler_params=pltpu.CompilerParams(
            collective_id=0, has_side_effects=True, vmem_limit_bytes=GRANT
        ),
        name="layer",
    )(*(pltpu.with_memory_space_constraint(v, pltpu.HBM) for v in (gain, g, u, d, x)))


def publish_kernel(wg, wu, wd, mixed, og, ou, od, om, sems):
    outs = [
        pltpu.make_async_copy(s, d, sems.at[i])
        for i, (s, d) in enumerate(((wg, og), (wu, ou), (wd, od), (mixed, om)))
    ]
    for c in outs:
        c.start()
    for c in outs:
        c.wait()


def publish(*arrays):
    vmem, any_ = pl.BlockSpec(memory_space=pltpu.VMEM), pl.BlockSpec(memory_space=pl.ANY)
    return pl.pallas_call(
        publish_kernel,
        out_shape=tuple(jax.ShapeDtypeStruct(a.shape, a.dtype) for a in arrays),
        in_specs=[vmem] * 4,
        out_specs=[any_] * 4,
        scratch_shapes=[pltpu.SemaphoreType.DMA((4,))],
        compiler_params=pltpu.CompilerParams(vmem_limit_bytes=1024 * 1024),
        name="publish",
    )(*arrays)


def solution(mesh):
    def on_device(tokens, norm_gain, gate_weight, up_weight, down_weight):
        wg, wu, wd, mixed = layer(mesh, norm_gain[None, :], gate_weight, up_weight, down_weight, tokens)
        og, ou, od, om = publish(wg, wu, wd, mixed)
        return (om, og, ou, od)

    return jax.shard_map(
        on_device,
        mesh=mesh,
        in_specs=(P("fs", None), P("fs"), P("fs", "tp"), P("fs", "tp"), P("fs", "tp")),
        out_specs=(P("fs", "tp"), P(None, "tp"), P(None, "tp"), P("tp", None)),
        check_vma=False,
    )
```

```python
import functools

import jax
import jax.numpy as jnp
from jax import lax
from jax.experimental import pallas as pl
from jax.experimental.pallas import tpu as pltpu
from jax.sharding import PartitionSpec as P

MESH = pl.DeviceIdType.MESH
GRANT = 26 * 1024 * 1024
CUTS = 4
W = 128


def lines(fs):
    y = 1
    while 2 * (2 * y) * (2 * y) <= fs:
        y *= 2
    return fs // y, y


def when(cond, fn):
    pl.when(cond)(fn)


def each(lo, hi, fn):
    if hi > lo:
        pl.loop(lo, hi)(fn)


def column_times(pq):
    tail = 4 * pq - 2 * pq - pq // 2
    return (
        [18 + 2 * (p % pq + 1) / pq for p in range(2 * pq)]
        + [20 + (i + 1) / (pq // 2) for i in range(pq // 2)]
        + [15 + 6 * (i + 1) / tail for i in range(tail)]
    )


def column_units(pq, nc, paired):
    times = column_times(pq) if paired else range(nc)
    if pq % 2:
        return (), tuple(sorted(range(nc), key=lambda p: times[p]))
    pairs = sorted(range(0, nc, 2), key=lambda p: max(times[p], times[p + 1]))
    ends = [p + i for p in pairs[-2:] for i in range(2)]
    return tuple(pairs[:-2]), tuple(sorted(ends, key=lambda p: times[p]))


def layer_kernel(
    Z, Y, T, nk, paired,
    gain_hbm, g_hbm, u_hbm, d_hbm, x_hbm,
    wg, wu, wd, mixed,
    gain_row, stage_g, stage_u, stage_d, own_d, transit, normed, hidden, part, near, pair, far,
    in_gain, in_g, in_u, in_d, in_x, s_up, s_dn, s_y, s_det, r_w, s_one, s_tz, s_tx, r_t,
    s_dz, s_dy, r_d, s_a, r_a, s_b, r_b,
):
    f, t = lax.axis_index("fs"), lax.axis_index("tp")
    X = T // 2
    z, y = f // Y, lax.rem(f, Y)
    x, core = t // 2, lax.rem(t, 2)
    has_up, has_dn = z < Z - 1, z > 0
    up, dn = (f + Y, t), (f - Y, t)
    others = [lax.rem(y + i, Y) for i in range(1, Y)]
    across = [(z * Y + o, t) for o in others]
    rows = g_hbm.shape[0]
    ck = rows // nk
    rows_d, cols_d = d_hbm.shape
    pq = cols_d // W
    nc = T * pq
    n = x_hbm.shape[0]
    staged, full = (stage_g, stage_u), (wg, wu)
    pieces = [(k, a) for k in range(nk) for a in range(2)]

    def load(k, a):
        at = pl.ds(k * ck, ck)
        return pltpu.make_async_copy((g_hbm, u_hbm)[a].at[at, :], staged[a].at[at, :], (in_g, in_u)[a].at[k])

    load_d = pltpu.make_async_copy(d_hbm, stage_d, in_d.at[0])
    load_x = pltpu.make_async_copy(x_hbm, normed, in_x.at[0])
    load_gain = pltpu.make_async_copy(gain_hbm, gain_row, in_gain.at[0])
    load_gain.start()
    for k, a in pieces:
        load(k, a).start()
    load_d.start()
    load_x.start()

    barrier = pltpu.get_barrier_semaphore()

    def greet(dev):
        pl.semaphore_signal(barrier, inc=1, device_id=dev, device_id_type=MESH)

    when(has_up, lambda: greet(up))
    when(has_dn, lambda: greet(dn))
    for dev in across:
        greet(dev)
    for i in range(1, T):
        greet((f, lax.rem(t + i, T)))

    load_gain.wait()
    diagonal = lax.broadcasted_iota(jnp.int32, (rows, rows), 0) == lax.broadcasted_iota(jnp.int32, (rows, rows), 1)
    gain = jnp.sum(jnp.where(diagonal, jnp.broadcast_to(gain_row[...], (rows, rows)), 0.0), axis=1, keepdims=True)

    def copy(src, dst, ss, rs, dev):
        return pltpu.make_async_remote_copy(
            src_ref=src, dst_ref=dst, send_sem=ss, recv_sem=rs, device_id=dev, device_id_type=MESH
        )

    def weight(a, k, source, ss, dev):
        at = full[a].at[pl.ds(pl.multiple_of(source * rows + k * ck, ck), ck), :]
        return copy(at, at, ss, r_w.at[source, a, k], dev)

    def arrived(a, k, source):
        weight(a, k, source, s_det.at[0], (f, lax.rem(t + 1, T))).wait_recv()

    def start(cond, make):
        if cond is None:
            make().start()
        else:
            when(cond, lambda: make().start())

    def scale(k, a):
        load(k, a).wait()
        at = pl.ds(pl.multiple_of(f * rows + k * ck, ck), ck)
        full[a][at, :] = (gain[k * ck:(k + 1) * ck, :] * staged[a][pl.ds(k * ck, ck), :]).astype(jnp.bfloat16)

    def send_own(k, a):
        start(has_up, lambda: weight(a, k, f, s_up.at[z], up))
        start(has_dn, lambda: weight(a, k, f, s_dn.at[z], dn))
        for i in range(Y - 1):
            start(None, lambda i=i: weight(a, k, f, s_y.at[i, z], across[i]))

    scale(*pieces[0])
    scale(*pieces[1])
    pl.semaphore_wait(barrier, Y + T - 2 + has_up.astype(jnp.int32) + has_dn.astype(jnp.int32))
    for i, piece in enumerate(pieces):
        if i + 2 < len(pieces):
            scale(*pieces[i + 2])
        send_own(*piece)

    def cols(j):
        return pl.ds(pl.multiple_of(j * W, W), W)

    def line_rows(line):
        return pl.ds(pl.multiple_of(line * rows_d, rows_d), rows_d)

    def down(line, j, ss, dev):
        at = wd.at[line_rows(line), cols(j)]
        return copy(at, at, ss, r_d.at[line, j], dev)

    def down_arrived(line, j):
        down(line, j, s_dy.at[0, 0], (f, lax.rem(t + 1, T))).wait_recv()

    load_d.wait()
    own_d[...] = stage_d[...].astype(jnp.bfloat16)

    @pl.when(z == t)
    def _():
        wd[line_rows(y), pl.ds(pl.multiple_of(t * cols_d, cols_d), cols_d)] = stage_d[...].astype(jnp.bfloat16)

    def first(p):
        return copy(
            own_d.at[:, pl.ds(p * W, W)], wd.at[line_rows(y), cols(t * pq + p)],
            s_one.at[0], r_d.at[y, t * pq + p], (f, z),
        )

    load_x.wait()
    slab = 64 if n % 64 == 0 else n

    def normalise(i):
        at = pl.ds(pl.multiple_of(i * slab, slab), slab)
        v = normed[at, :].astype(jnp.float32)
        normed[at, :] = (v * lax.rsqrt(jnp.mean(v * v, axis=1, keepdims=True) + 1e-05)).astype(jnp.bfloat16)

    normalise(0)
    for p in range(pq):
        start(z != t, lambda p=p: first(p))
    each(1, n // slab, normalise)

    at_home = z == t
    can_up = jnp.logical_and(has_up, z >= t)
    can_dn = jnp.logical_and(has_dn, z <= t)
    inner = jnp.logical_and(has_up, has_dn)
    if paired:
        half = t // (T // 2)
        shift = (nc // 2) * (1 - half)
        far_up, far_dn = half == 0, half == 1
        beyond = jnp.logical_or(jnp.logical_and(z < t, far_dn), jnp.logical_and(z > t, far_up))
        fwd_mid = jnp.logical_or(
            jnp.logical_and(can_up, jnp.logical_not(far_up)), jnp.logical_and(can_dn, jnp.logical_not(far_dn))
        )
        mid_lo, mid_hi = 2 * pq, 2 * pq + pq // 2
    else:
        shift = 0
        mid_lo, mid_hi = 0, nc
    fwd_all = jnp.logical_or(can_up, can_dn)
    if paired:
        passes = jnp.logical_or(fwd_all, beyond)
    away = jnp.logical_not(at_home)

    def column(r):
        return lax.rem(r + shift, nc)

    def turned(r):
        return lax.rem(r + (nc // 2) * (z >= Z // 2).astype(jnp.int32), nc) if paired else r

    def pick(table, i):
        return turned(sum(p * (i == e).astype(jnp.int32) for e, p in enumerate(table)))

    pair_units, last_units = column_units(pq, nc, paired)
    sequence = [p + i for p in pair_units for i in range(2)] + list(last_units)

    def piece_of(i):
        return pick(sequence, i)

    bent = (pq if paired else 0, lambda i: column(core * pq + i), 0)
    low = (pq if paired else 0, lambda i: column((1 - core) * pq + i), 1)
    mid = (mid_hi - mid_lo, lambda i: column(mid_lo + i), 1)
    high = (nc - mid_hi, lambda i: column(mid_hi + i), 2)
    sizes = (bent[0], low[0] + mid[0], high[0])

    def over(kind, fn):
        each(0, kind[0], lambda i: fn(kind[1](i), kind[2]))

    def both(a, b):
        return jnp.logical_and(a, b)

    def kinds(j):
        r = lax.rem(j - shift + nc, nc)
        is_high = r >= mid_hi
        is_bent = both(r < 2 * pq, r // pq == core)
        return is_high, is_bent, jnp.logical_not(jnp.logical_or(is_high, is_bent))

    def z_send(line, j, kind, which, direction):
        return down(line, j, s_dz.at[direction, which, kind], (up, dn)[direction])

    def near_ok(direction):
        return jnp.logical_not((far_up, far_dn)[direction])

    def can(direction):
        return (can_up, can_dn)[direction]

    def cross(j, kind):
        for i in range(Y - 1):
            down(y, j, s_dy.at[i, kind], across[i]).start()

    other = others[0]

    def assemble():
        for i in range(1, T):
            owner = lax.rem(t + i, T)
            for p in range(pq):
                down_arrived(y, owner * pq + p)
        over(high, cross)
        if paired:
            @pl.when(inner)
            def _():
                over(low, cross)
                over(mid, cross)

    if paired:
        guest = lax.rem(t + T // 2, T)
        guest_dn = guest // (T // 2) == 1
        guest_here = jnp.logical_or(both(z < guest, guest_dn), both(z > guest, jnp.logical_not(guest_dn)))
        guest_on = (both(both(z >= guest, has_up), jnp.logical_not(guest_dn)), both(both(z <= guest, has_dn), guest_dn))

        def relay(p, direction, src):
            return copy(
                src.at[:, cols(p)], transit.at[:, cols(p)], s_tz.at[0], r_t.at[p], (up, dn)[direction]
            )

        def hand_over(p):
            return copy(
                transit.at[:, cols(p)], wd.at[line_rows(y), cols(t * pq + p)], s_tx.at[0], r_d.at[y, t * pq + p], (f, guest)
            )

    def leave(direction):
        if paired:
            @pl.when(both(z == guest, guest_on[direction]))
            def _():
                each(0, pq, lambda p: relay(p, direction, own_d).start())

        here = both(at_home, can(direction))
        if paired:
            here = both(here, jnp.logical_not(near_ok(direction)))

        @pl.when(here)
        def _():
            for kind in (low, mid, high):
                over(kind, lambda j, c: z_send(y, j, c, 0, direction).start())

    def hook(s):
        when(z == s, lambda: leave(0))
        when(z == Z - 1 - s, lambda: leave(1))

    for step in range(1, Z):
        for count, (k, a) in enumerate(pieces):
            if step == 1 and count == len(pieces) // 2:
                when(at_home, assemble)
            for sign in (-1, 1):
                zs = z + sign * step
                source = zs * Y + y
                valid = zs >= 0 if sign < 0 else zs < Z
                onward = jnp.logical_and(valid, has_up if sign < 0 else has_dn)
                when(valid, lambda a=a, k=k, s=source: arrived(a, k, s))
                if sign < 0:
                    start(onward, lambda a=a, k=k, s=source, q=zs: weight(a, k, s, s_up.at[q], up))
                else:
                    start(onward, lambda a=a, k=k, s=source, q=zs: weight(a, k, s, s_dn.at[q], dn))
                crossing = valid
                if paired and step == 1:
                    crossing = both(valid, zs != (0 if sign < 0 else Z - 1))
                for i in range(Y - 1):
                    start(crossing, lambda a=a, k=k, s=source, q=zs, i=i: weight(a, k, s, s_y.at[i, q], across[i]))
        if step == 1:
            hook(0)
            if paired:
                ends = jnp.logical_not(inner)
                beside = across[0][0]
                for k, a in pieces:
                    when(ends, lambda a=a, k=k: arrived(a, k, beside))
                    start(both(ends, has_up), lambda a=a, k=k: weight(a, k, beside, s_det.at[0], up))
                    start(both(ends, has_dn), lambda a=a, k=k: weight(a, k, beside, s_det.at[0], dn))
        hook(step)

    if paired:
        @pl.when(at_home)
        def _():
            @pl.when(jnp.logical_not(inner))
            def _():
                def late(i):
                    j = piece_of(i)
                    is_high, is_bent, is_mid = kinds(j)
                    when(jnp.logical_not(is_high), lambda: cross(j, is_mid.astype(jnp.int32)))
                each(0, nc, late)
            when(inner, lambda: over(bent, cross))

    else:
        when(at_home, lambda: over(mid, cross))

    if paired:
        @pl.when(guest_here)
        def _():
            def pass_on(p):
                copy(
                    transit.at[:, cols(p)], transit.at[:, cols(p)], s_tz.at[0], r_t.at[p], (f, guest)
                ).wait_recv()
                for direction in range(2):
                    when(guest_on[direction], lambda: relay(p, direction, transit).start())
                hand_over(p).start()
            each(0, pq, pass_on)

    if paired:
        @pl.when(both(at_home, inner))
        def _():
            def near_first(j, kind):
                for direction in range(2):
                    when(near_ok(direction), lambda: z_send(y, j, kind, 0, direction).start())
            over(bent, near_first)

            def near_pair(i):
                j = piece_of(i)
                is_high, is_bent, _ = kinds(j)
                kind = 1 + is_high.astype(jnp.int32)

                @pl.when(jnp.logical_not(is_bent))
                def _():
                    near_first(j, kind)
                    down_arrived(other, j)
                    for direction in range(2):
                        when(jnp.logical_or(near_ok(direction), is_high), lambda: z_send(other, j, kind, 1, direction).start())
            each(0, nc, near_pair)

    @pl.when(away)
    def _():
        def bend(j, kind):
            down_arrived(y, j)
            for direction in range(2):
                when(both(can(direction), near_ok(direction)), lambda: z_send(y, j, kind, 0, direction).start())
            cross(j, kind)

        def straight(j, kind):
            down_arrived(y, j)
            for direction in range(2):
                when(can(direction), lambda: z_send(y, j, kind, 0, direction).start())
            if paired:
                when(beyond, lambda: cross(j, kind))
            else:
                cross(j, kind)

        over(bent, bend)
        if paired:
            @pl.when(passes)
            def _():
                over(low, straight)
                over(mid, straight)
        else:
            over(mid, straight)

    if paired:
        @pl.when(both(fwd_mid, away))
        def _():
            def twin(j, kind):
                down_arrived(other, j)
                for direction in range(2):
                    when(both(can(direction), near_ok(direction)), lambda: z_send(other, j, kind, 1, direction).start())
            over(low, twin)
            over(mid, twin)

        @pl.when(both(fwd_all, jnp.logical_or(away, jnp.logical_not(inner))))
        def _():
            def twins(j, kind):
                @pl.when(away)
                def _():
                    down_arrived(y, j)
                    for direction in range(2):
                        when(can(direction), lambda: z_send(y, j, kind, 0, direction).start())
                down_arrived(other, j)
                for direction in range(2):
                    when(can(direction), lambda: z_send(other, j, kind, 1, direction).start())
            over(high, twins)

    for zs in range(Z):
        for o in others:
            for k, a in pieces:
                if paired and zs in (0, Z - 1):
                    when(zs != z, lambda a=a, k=k, zs=zs, o=o: arrived(a, k, zs * Y + o))
                else:
                    arrived(a, k, zs * Y + o)
    units = wg.shape[1]
    width = 256 if units % 256 == 0 else 128

    @pl.loop(0, units // width)
    def _(j):
        at = pl.ds(pl.multiple_of(j * width, width), width)
        gate = jnp.dot(normed[...], wg[:, at], preferred_element_type=jnp.float32)
        up_ = jnp.dot(normed[...], wu[:, at], preferred_element_type=jnp.float32)
        hidden[:, at] = (gate / (1.0 + jnp.exp(-gate)) * up_).astype(jnp.bfloat16)

    def drained(sem):
        both_shards = wg.at[pl.ds(0, 2 * rows), :]
        copy(both_shards, both_shards, sem, r_w.at[0, 0, 0], (f, lax.rem(t + 1, T))).wait_send()

    for q in range(Z):
        when(jnp.logical_and(has_up, q <= z), lambda q=q: drained(s_up.at[q]))
        when(jnp.logical_and(has_dn, q >= z), lambda q=q: drained(s_dn.at[q]))
        crossing = z >= 0
        if paired and q in (0, Z - 1):
            crossing = z != (1 if q == 0 else Z - 2)
        for i in range(Y - 1):
            when(crossing, lambda q=q, i=i: drained(s_y.at[i, q]))
    if paired:
        when(jnp.logical_not(inner), lambda: drained(s_det.at[0]))

    mate = (f, x * 2 + 1 - core)

    def span(j, count):
        return pl.ds(pl.multiple_of(j * W, W), count * W)

    def to_mate(j, count):
        return copy(part.at[:, span(j, count)], near.at[:, span(j, count)], s_a.at[0], r_a.at[j], mate)

    def to_owner(j, count, slot, dev):
        p = lax.rem(j, pq)
        return copy(pair.at[:, span(j, count)], far.at[slot, :, span(p, count)], s_b.at[0], r_b.at[slot, p], dev)

    def whole(j):
        if paired:
            is_high, is_bent, is_mid = kinds(j)
            late = both(is_high, jnp.logical_not(fwd_all))
            late_own = both(away, jnp.logical_or(late, both(is_mid, jnp.logical_not(passes))))
            when(late_own, lambda: down_arrived(y, j))
            late_other = jnp.logical_or(jnp.logical_or(late, is_bent), both(is_mid, jnp.logical_not(fwd_mid)))
            when(late_other, lambda: down_arrived(other, j))
        else:
            for o in others:
                down_arrived(o, j)

    def ours(j):
        return lax.rem(j // pq, 2) == core

    def abroad(j):
        return both(ours(j), j // pq // 2 != x)

    def products(table, count, lag):
        m = len(table)

        def multiply(j):
            for i in range(count):
                whole(j + i)
            at = span(j, count)
            part[:, at] = jnp.dot(hidden[...], wd[:, at], preferred_element_type=jnp.float32).astype(jnp.bfloat16)

        def add(j):
            at = span(j, count)
            when(ours(j), lambda: to_mate(j, count).wait_recv())

            @pl.when(abroad(j))
            def _():
                pair[:, at] = (part[:, at].astype(jnp.float32) + near[:, at].astype(jnp.float32)).astype(jnp.bfloat16)

        def ship(j):
            owner = j // pq
            to_owner(j, count, lax.rem(x - owner // 2 + X, X) - 1, (f, owner)).start()

        def step(i):
            now, then = i < m, i >= lag
            j0 = pick(table, jnp.minimum(i, m - 1))
            j1 = pick(table, jnp.maximum(i - lag, 0))
            if lag == 1:
                when(then, lambda: add(j1))
                when(both(then, abroad(j1)), lambda: ship(j1))
                when(now, lambda: multiply(j0))
                when(both(now, jnp.logical_not(ours(j0))), lambda: to_mate(j0, count).start())
            else:
                when(now, lambda: multiply(j0))
                when(then, lambda: add(j1))
                when(both(now, jnp.logical_not(ours(j0))), lambda: to_mate(j0, count).start())
                when(both(then, abroad(j1)), lambda: ship(j1))

        each(0, m + lag, step)

    def finish(table, count):
        def step(i):
            j = pick(table, i)

            @pl.when(j // pq == t)
            def _():
                at, to = span(j, count), span(lax.rem(j, pq), count)
                acc = part[:, at].astype(jnp.float32) + near[:, at].astype(jnp.float32)
                for slot in range(X - 1):
                    to_owner(j, count, slot, mate).wait_recv()
                    acc = acc + far[slot, :, to].astype(jnp.float32)
                mixed[:, to] = acc.astype(mixed.dtype)

        each(0, len(table), step)

    if pair_units:
        products(pair_units, 2, 2)
    products(last_units, 1, 1)
    if pair_units:
        finish(pair_units, 2)

    def gone(sem, ref):
        copy(ref, ref, sem, r_a.at[0], mate).wait_send()

    def gone_down(sem, kind):
        if sizes[kind]:
            gone(sem, wd.at[pl.ds(0, rows_d), pl.ds(0, sizes[kind] * W)])

    when(away, lambda: gone(s_one.at[0], own_d))
    if paired:
        when(jnp.logical_or(guest_on[0], guest_on[1]), lambda: gone(s_tz.at[0], transit))
        when(guest_here, lambda: gone(s_tx.at[0], transit))
    for direction in range(2):
        if paired:
            near_dir = both(can(direction), near_ok(direction))
            when(near_dir, lambda: gone_down(s_dz.at[direction, 0, 0], 0))
            when(near_dir, lambda: gone_down(s_dz.at[direction, 1, 1], 1))
            when(can(direction), lambda: gone_down(s_dz.at[direction, 0, 2], 2))
            when(can(direction), lambda: gone_down(s_dz.at[direction, 1, 2], 2))
        when(can(direction), lambda: gone_down(s_dz.at[direction, 0, 1], 1))
    for i in range(Y - 1):
        if paired:
            gone_down(s_dy.at[i, 0], 0)
            when(jnp.logical_or(at_home, beyond), lambda: gone_down(s_dy.at[i, 1], 1))
            when(at_home, lambda: gone_down(s_dy.at[i, 2], 2))
        else:
            gone_down(s_dy.at[i, 1], 1)
    finish(last_units, 1)
    gone(s_a.at[0], part.at[:, pl.ds(0, nc * W // 2)])
    gone(s_b.at[0], pair.at[:, pl.ds(0, (X - 1) * pq * W)])


def layer(mesh, gain, g, u, d, x):
    fs, T = mesh.shape["fs"], mesh.shape["tp"]
    Z, Y = lines(fs)
    X = T // 2
    rows, rows_d, n = g.shape[0], d.shape[0], x.shape[0]
    pq = d.shape[1] // W
    nc = T * pq
    nk = max(1, min(4, rows // 64))
    paired = Y == 2 and X == 2 and Z == T and pq % 2 == 0
    lanes = max(Y - 1, 1)
    dma = pltpu.SemaphoreType.DMA
    vmem, hbm = pl.BlockSpec(memory_space=pltpu.VMEM), pl.BlockSpec(memory_space=pltpu.HBM)
    bf = jnp.bfloat16
    return pl.pallas_call(
        functools.partial(layer_kernel, Z, Y, T, nk, paired),
        out_shape=(
            jax.ShapeDtypeStruct((rows * fs, g.shape[1]), bf),
            jax.ShapeDtypeStruct((rows * fs, g.shape[1]), bf),
            jax.ShapeDtypeStruct((rows_d * Y, d.shape[1] * T), bf),
            jax.ShapeDtypeStruct((n, d.shape[1]), bf),
        ),
        in_specs=[hbm] * 5,
        out_specs=[vmem] * 4,
        scratch_shapes=[
            pltpu.VMEM(gain.shape, jnp.float32),
            pltpu.VMEM(g.shape, jnp.float32), pltpu.VMEM(u.shape, jnp.float32), pltpu.VMEM(d.shape, jnp.float32),
            pltpu.VMEM(d.shape, bf), pltpu.VMEM(d.shape, bf), pltpu.VMEM(x.shape, bf), pltpu.VMEM((n, g.shape[1]), bf),
            pltpu.VMEM((n, nc * W), bf), pltpu.VMEM((n, nc * W), bf), pltpu.VMEM((n, nc * W), bf),
            pltpu.VMEM((max(X - 1, 1), n, pq * W), bf),
            dma((1,)), dma((nk,)), dma((nk,)), dma((1,)), dma((1,)),
            dma((Z,)), dma((Z,)), dma((lanes, Z)), dma((1,)), dma((fs, 2, nk)),
            dma((1,)), dma((1,)), dma((1,)), dma((pq,)),
            dma((2, 2, 3)), dma((lanes, 3)), dma((Y, nc)),
            dma((1,)), dma((nc,)), dma((1,)), dma((max(X - 1, 1), pq)),
        ],
        compiler_params=pltpu.CompilerParams(
            collective_id=0, has_side_effects=True, vmem_limit_bytes=GRANT
        ),
        name="layer",
    )(*(pltpu.with_memory_space_constraint(v, pltpu.HBM) for v in (gain, g, u, d, x)))


def publish_kernel(cuts, wg, wu, wd, mixed, og, ou, od, om, sems):
    outs = []
    for a, (s, d) in enumerate(((wg, og), (wu, ou), (wd, od), (mixed, om))):
        h = s.shape[0] // cuts
        for i in range(cuts):
            outs.append(pltpu.make_async_copy(s.at[pl.ds(i * h, h), :], d.at[pl.ds(i * h, h), :], sems.at[a, i]))
    for c in outs:
        c.start()
    for c in outs:
        c.wait()


def publish(*arrays):
    vmem, any_ = pl.BlockSpec(memory_space=pltpu.VMEM), pl.BlockSpec(memory_space=pl.ANY)
    return pl.pallas_call(
        functools.partial(publish_kernel, CUTS),
        out_shape=tuple(jax.ShapeDtypeStruct(a.shape, a.dtype) for a in arrays),
        in_specs=[vmem] * 4,
        out_specs=[any_] * 4,
        scratch_shapes=[pltpu.SemaphoreType.DMA((4, CUTS))],
        compiler_params=pltpu.CompilerParams(vmem_limit_bytes=1024 * 1024),
        name="publish",
    )(*arrays)


def solution(mesh):
    def on_device(tokens, norm_gain, gate_weight, up_weight, down_weight):
        wg, wu, wd, mixed = layer(mesh, norm_gain[None, :], gate_weight, up_weight, down_weight, tokens)
        og, ou, od, om = publish(wg, wu, wd, mixed)
        return (om, og, ou, od)

    return jax.shard_map(
        on_device,
        mesh=mesh,
        in_specs=(P("fs", None), P("fs"), P("fs", "tp"), P("fs", "tp"), P("fs", "tp")),
        out_specs=(P("fs", "tp"), P(None, "tp"), P(None, "tp"), P("tp", None)),
        check_vma=False,
    )
```

```python
import functools

import jax
import jax.numpy as jnp
from jax import lax
from jax.experimental import pallas as pl
from jax.experimental.pallas import tpu as pltpu
from jax.sharding import PartitionSpec as P

MESH = pl.DeviceIdType.MESH
GRANT = 26 * 1024 * 1024
CUTS = 4
W = 128


def lines(fs):
    y = 1
    while 2 * (2 * y) * (2 * y) <= fs:
        y *= 2
    return fs // y, y


def when(cond, fn):
    pl.when(cond)(fn)


def each(lo, hi, fn):
    if hi > lo:
        pl.loop(lo, hi)(fn)


def column_times(pq):
    tail = 4 * pq - 2 * pq - pq // 2
    return (
        [18 + 2 * (p % pq + 1) / pq for p in range(2 * pq)]
        + [20 + (i + 1) / (pq // 2) for i in range(pq // 2)]
        + [15 + 6 * (i + 1) / tail for i in range(tail)]
    )


def column_units(pq, nc, paired):
    times = column_times(pq) if paired else range(nc)
    if pq % 2:
        return (), tuple(sorted(range(nc), key=lambda p: times[p]))
    pairs = sorted(range(0, nc, 2), key=lambda p: max(times[p], times[p + 1]))
    ends = [p + i for p in pairs[-2:] for i in range(2)]
    return tuple(pairs[:-2]), tuple(sorted(ends, key=lambda p: (times[p], -p)))


def layer_kernel(
    Z, Y, T, nk, paired,
    gain_hbm, g_hbm, u_hbm, d_hbm, x_hbm,
    wg, wu, wd, mixed,
    gain_row, stage_g, stage_u, stage_d, own_d, transit, normed, hidden, part, near, pair, far,
    in_gain, in_g, in_u, in_d, in_x, s_up, s_dn, s_y, s_det, r_w, r_o, s_one, s_tz, s_tx, r_t,
    s_dz, s_dy, r_d, s_a, r_a, s_b, r_b, r_c,
):
    f, t = lax.axis_index("fs"), lax.axis_index("tp")
    X = T // 2
    z, y = f // Y, lax.rem(f, Y)
    x, core = t // 2, lax.rem(t, 2)
    has_up, has_dn = z < Z - 1, z > 0
    up, dn = (f + Y, t), (f - Y, t)
    others = [lax.rem(y + i, Y) for i in range(1, Y)]
    across = [(z * Y + o, t) for o in others]
    rows = g_hbm.shape[0]
    ck = rows // nk
    rows_d, cols_d = d_hbm.shape
    pq = cols_d // W
    nc = T * pq
    n = x_hbm.shape[0]
    staged, full = (stage_g, stage_u), (wg, wu)
    pieces = [(k, a) for k in range(nk) for a in range(2)]

    def load(k, a):
        at = pl.ds(k * ck, ck)
        return pltpu.make_async_copy((g_hbm, u_hbm)[a].at[at, :], staged[a].at[at, :], (in_g, in_u)[a].at[k])

    load_d = pltpu.make_async_copy(d_hbm, stage_d, in_d.at[0])
    load_x = pltpu.make_async_copy(x_hbm, normed, in_x.at[0])
    load_gain = pltpu.make_async_copy(gain_hbm, gain_row, in_gain.at[0])
    load_gain.start()
    for k, a in pieces:
        load(k, a).start()
    load_d.start()
    load_x.start()

    barrier = pltpu.get_barrier_semaphore()

    def greet(dev):
        pl.semaphore_signal(barrier, inc=1, device_id=dev, device_id_type=MESH)

    when(has_up, lambda: greet(up))
    when(has_dn, lambda: greet(dn))
    for dev in across:
        greet(dev)
    for i in range(1, T):
        greet((f, lax.rem(t + i, T)))

    load_gain.wait()
    diagonal = lax.broadcasted_iota(jnp.int32, (rows, rows), 0) == lax.broadcasted_iota(jnp.int32, (rows, rows), 1)
    gain = jnp.sum(jnp.where(diagonal, jnp.broadcast_to(gain_row[...], (rows, rows)), 0.0), axis=1, keepdims=True)

    def copy(src, dst, ss, rs, dev):
        return pltpu.make_async_remote_copy(
            src_ref=src, dst_ref=dst, send_sem=ss, recv_sem=rs, device_id=dev, device_id_type=MESH
        )

    def weight(a, k, source, ss, rs, dev):
        at = full[a].at[pl.ds(pl.multiple_of(source * rows + k * ck, ck), ck), :]
        return copy(at, at, ss, rs, dev)

    def along(a, k, source, ss, dev):
        return weight(a, k, source, ss, r_w.at[source // Y, k], dev)

    def beyond_line(a, k, source, ss, dev):
        return weight(a, k, source, ss, r_o.at[source], dev)

    def taken(height, ss, rs):
        at = wg.at[pl.ds(0, height), :]
        return copy(at, at, ss, rs, (f, lax.rem(t + 1, T)))

    def arrived(k, source):
        taken(2 * ck, s_det.at[0], r_w.at[source // Y, k]).wait_recv()

    def arrived_whole(source):
        taken(2 * rows, s_det.at[0], r_o.at[source]).wait_recv()

    def start(cond, make):
        if cond is None:
            make().start()
        else:
            when(cond, lambda: make().start())

    def scale(k, a):
        load(k, a).wait()
        at = pl.ds(pl.multiple_of(f * rows + k * ck, ck), ck)
        full[a][at, :] = (gain[k * ck:(k + 1) * ck, :] * staged[a][pl.ds(k * ck, ck), :]).astype(jnp.bfloat16)

    def send_own(k, a):
        start(has_up, lambda: along(a, k, f, s_up.at[0], up))
        start(has_dn, lambda: along(a, k, f, s_dn.at[0], dn))
        for i in range(Y - 1):
            start(None, lambda i=i: beyond_line(a, k, f, s_y.at[i], across[i]))

    scale(*pieces[0])
    scale(*pieces[1])
    pl.semaphore_wait(barrier, Y + T - 2 + has_up.astype(jnp.int32) + has_dn.astype(jnp.int32))
    for i, piece in enumerate(pieces):
        if i + 2 < len(pieces):
            scale(*pieces[i + 2])
        send_own(*piece)

    def cols(j):
        return pl.ds(pl.multiple_of(j * W, W), W)

    def line_rows(line):
        return pl.ds(pl.multiple_of(line * rows_d, rows_d), rows_d)

    def down(line, j, ss, dev):
        at = wd.at[line_rows(line), cols(j)]
        return copy(at, at, ss, r_d.at[line, j], dev)

    def down_arrived(line, j):
        down(line, j, s_dy.at[0], (f, lax.rem(t + 1, T))).wait_recv()

    load_d.wait()
    own_d[...] = stage_d[...].astype(jnp.bfloat16)

    @pl.when(z == t)
    def _():
        wd[line_rows(y), pl.ds(pl.multiple_of(t * cols_d, cols_d), cols_d)] = stage_d[...].astype(jnp.bfloat16)

    def first(p):
        return copy(
            own_d.at[:, pl.ds(p * W, W)], wd.at[line_rows(y), cols(t * pq + p)],
            s_one.at[0], r_d.at[y, t * pq + p], (f, z),
        )

    load_x.wait()
    slab = 64 if n % 64 == 0 else n

    def normalise(i):
        at = pl.ds(pl.multiple_of(i * slab, slab), slab)
        v = normed[at, :].astype(jnp.float32)
        normed[at, :] = (v * lax.rsqrt(jnp.mean(v * v, axis=1, keepdims=True) + 1e-05)).astype(jnp.bfloat16)

    normalise(0)
    for p in range(pq):
        start(z != t, lambda p=p: first(p))
    each(1, n // slab, normalise)

    at_home = z == t
    can_up = jnp.logical_and(has_up, z >= t)
    can_dn = jnp.logical_and(has_dn, z <= t)
    inner = jnp.logical_and(has_up, has_dn)
    if paired:
        half = t // (T // 2)
        shift = (nc // 2) * (1 - half)
        far_up, far_dn = half == 0, half == 1
        beyond = jnp.logical_or(jnp.logical_and(z < t, far_dn), jnp.logical_and(z > t, far_up))
        fwd_mid = jnp.logical_or(
            jnp.logical_and(can_up, jnp.logical_not(far_up)), jnp.logical_and(can_dn, jnp.logical_not(far_dn))
        )
        mid_lo, mid_hi = 2 * pq, 2 * pq + pq // 2
    else:
        shift = 0
        mid_lo, mid_hi = 0, nc
    fwd_all = jnp.logical_or(can_up, can_dn)
    if paired:
        passes = jnp.logical_or(fwd_all, beyond)
    away = jnp.logical_not(at_home)

    def column(r):
        return lax.rem(r + shift, nc)

    def turned(r):
        return lax.rem(r + (nc // 2) * (z >= Z // 2).astype(jnp.int32), nc) if paired else r

    def pick(table, i):
        return turned(sum(p * (i == e).astype(jnp.int32) for e, p in enumerate(table)))

    pair_units, last_units = column_units(pq, nc, paired)
    sequence = [p + i for p in pair_units for i in range(2)] + list(last_units)

    def piece_of(i):
        return pick(sequence, i)

    bent = (pq if paired else 0, lambda i: column(core * pq + i))
    low = (pq if paired else 0, lambda i: column((1 - core) * pq + i))
    mid = (mid_hi - mid_lo, lambda i: column(mid_lo + i))
    high = (nc - mid_hi, lambda i: column(mid_hi + i))

    def over(kind, fn):
        each(0, kind[0], lambda i: fn(kind[1](i)))

    def both(a, b):
        return jnp.logical_and(a, b)

    def kinds(j):
        r = lax.rem(j - shift + nc, nc)
        is_high = r >= mid_hi
        is_bent = both(r < 2 * pq, r // pq == core)
        return is_high, is_bent, jnp.logical_not(jnp.logical_or(is_high, is_bent))

    def z_send(line, j, direction):
        return down(line, j, s_dz.at[direction], (up, dn)[direction])

    def near_ok(direction):
        return jnp.logical_not((far_up, far_dn)[direction])

    def can(direction):
        return (can_up, can_dn)[direction]

    def cross(j):
        for i in range(Y - 1):
            down(y, j, s_dy.at[i], across[i]).start()

    other = others[0]

    def assemble():
        for i in range(1, T):
            owner = lax.rem(t + i, T)
            for p in range(pq):
                down_arrived(y, owner * pq + p)
        over(high, cross)
        if paired:
            @pl.when(inner)
            def _():
                over(low, cross)
                over(mid, cross)

    if paired:
        guest = lax.rem(t + T // 2, T)
        guest_dn = guest // (T // 2) == 1
        guest_here = jnp.logical_or(both(z < guest, guest_dn), both(z > guest, jnp.logical_not(guest_dn)))
        guest_on = (both(both(z >= guest, has_up), jnp.logical_not(guest_dn)), both(both(z <= guest, has_dn), guest_dn))

        def relay(p, direction, src):
            return copy(
                src.at[:, cols(p)], transit.at[:, cols(p)], s_tz.at[0], r_t.at[p], (up, dn)[direction]
            )

        def hand_over(p):
            return copy(
                transit.at[:, cols(p)], wd.at[line_rows(y), cols(t * pq + p)], s_tx.at[0], r_d.at[y, t * pq + p], (f, guest)
            )

    def leave(direction):
        if paired:
            @pl.when(both(z == guest, guest_on[direction]))
            def _():
                each(0, pq, lambda p: relay(p, direction, own_d).start())

        here = both(at_home, can(direction))
        if paired:
            here = both(here, jnp.logical_not(near_ok(direction)))

        @pl.when(here)
        def _():
            for kind in (low, mid, high):
                over(kind, lambda j: z_send(y, j, direction).start())

    def hook(s):
        when(z == s, lambda: leave(0))
        when(z == Z - 1 - s, lambda: leave(1))

    for step in range(1, Z):
        for k in range(nk):
            if step == 1 and k == nk // 2:
                when(at_home, assemble)
            for sign in (-1, 1):
                zs = z + sign * step
                source = zs * Y + y
                valid = zs >= 0 if sign < 0 else zs < Z
                onward = jnp.logical_and(valid, has_up if sign < 0 else has_dn)
                crossing = valid
                if paired and step == 1:
                    crossing = both(valid, zs != (0 if sign < 0 else Z - 1))
                when(valid, lambda k=k, s=source: arrived(k, s))
                for a in range(2):
                    if sign < 0:
                        start(onward, lambda a=a, k=k, s=source: along(a, k, s, s_up.at[0], up))
                    else:
                        start(onward, lambda a=a, k=k, s=source: along(a, k, s, s_dn.at[0], dn))
                    for i in range(Y - 1):
                        start(crossing, lambda a=a, k=k, s=source, i=i: beyond_line(a, k, s, s_y.at[i], across[i]))
        if step == 1:
            hook(0)
            if paired:
                ends = jnp.logical_not(inner)
                beside = across[0][0]
                when(ends, lambda: arrived_whole(beside))
                for k, a in pieces:
                    start(both(ends, has_up), lambda a=a, k=k: beyond_line(a, k, beside, s_det.at[0], up))
                    start(both(ends, has_dn), lambda a=a, k=k: beyond_line(a, k, beside, s_det.at[0], dn))
        hook(step)

    if paired:
        @pl.when(at_home)
        def _():
            @pl.when(jnp.logical_not(inner))
            def _():
                def late(i):
                    j = piece_of(i)
                    is_high, _, _ = kinds(j)
                    when(jnp.logical_not(is_high), lambda: cross(j))
                each(0, nc, late)
            when(inner, lambda: over(bent, cross))

    else:
        when(at_home, lambda: over(mid, cross))

    if paired:
        @pl.when(guest_here)
        def _():
            def pass_on(p):
                copy(
                    transit.at[:, cols(p)], transit.at[:, cols(p)], s_tz.at[0], r_t.at[p], (f, guest)
                ).wait_recv()
                for direction in range(2):
                    when(guest_on[direction], lambda: relay(p, direction, transit).start())
                hand_over(p).start()
            each(0, pq, pass_on)

    if paired:
        @pl.when(both(at_home, inner))
        def _():
            def near_first(j):
                for direction in range(2):
                    when(near_ok(direction), lambda: z_send(y, j, direction).start())
            over(bent, near_first)

            def near_pair(i):
                j = piece_of(i)
                is_high, is_bent, _ = kinds(j)

                @pl.when(jnp.logical_not(is_bent))
                def _():
                    near_first(j)
                    down_arrived(other, j)
                    for direction in range(2):
                        when(jnp.logical_or(near_ok(direction), is_high), lambda: z_send(other, j, direction).start())
            each(0, nc, near_pair)

    @pl.when(away)
    def _():
        def bend(j):
            down_arrived(y, j)
            for direction in range(2):
                when(both(can(direction), near_ok(direction)), lambda: z_send(y, j, direction).start())
            cross(j)

        def straight(j):
            down_arrived(y, j)
            for direction in range(2):
                when(can(direction), lambda: z_send(y, j, direction).start())
            if paired:
                when(beyond, lambda: cross(j))
            else:
                cross(j)

        over(bent, bend)
        if paired:
            @pl.when(passes)
            def _():
                over(low, straight)
                over(mid, straight)
        else:
            over(mid, straight)

    if paired:
        @pl.when(both(fwd_mid, away))
        def _():
            def twin(j):
                down_arrived(other, j)
                for direction in range(2):
                    when(both(can(direction), near_ok(direction)), lambda: z_send(other, j, direction).start())
            over(low, twin)
            over(mid, twin)

        @pl.when(both(fwd_all, jnp.logical_or(away, jnp.logical_not(inner))))
        def _():
            def twins(j):
                @pl.when(away)
                def _():
                    down_arrived(y, j)
                    for direction in range(2):
                        when(can(direction), lambda: z_send(y, j, direction).start())
                down_arrived(other, j)
                for direction in range(2):
                    when(can(direction), lambda: z_send(other, j, direction).start())
            over(high, twins)

    for zs in range(Z):
        for o in others:
            if paired and zs in (0, Z - 1):
                when(zs != z, lambda zs=zs, o=o: arrived_whole(zs * Y + o))
            else:
                arrived_whole(zs * Y + o)
    units = wg.shape[1]
    width = 256 if units % 256 == 0 else 128

    @pl.loop(0, units // width)
    def _(j):
        at = pl.ds(pl.multiple_of(j * width, width), width)
        gate = jnp.dot(normed[...], wg[:, at], preferred_element_type=jnp.float32)
        up_ = jnp.dot(normed[...], wu[:, at], preferred_element_type=jnp.float32)
        hidden[:, at] = (gate / (1.0 + jnp.exp(-gate)) * up_).astype(jnp.bfloat16)

    def drained(cond, shards, sem):
        when(cond, lambda: taken(2 * rows * shards, sem, r_w.at[0, 0]).wait_send())

    for q in range(Z - 1):
        drained(z == q, q + 1, s_up.at[0])
        drained(z == Z - 1 - q, q + 1, s_dn.at[0])
    for i in range(Y - 1):
        if paired:
            drained(inner, Z - 1, s_y.at[i])
            drained(jnp.logical_not(inner), Z, s_y.at[i])
        else:
            drained(z >= 0, Z, s_y.at[i])
    if paired:
        drained(jnp.logical_not(inner), 1, s_det.at[0])

    mate = (f, x * 2 + 1 - core)

    def span(j, count):
        return pl.ds(pl.multiple_of(j * W, W), count * W)

    def height(half, halves):
        return pl.ds(pl.multiple_of(half * (n // halves), n // halves), n // halves)

    def to_mate(j, count, half, halves, unit):
        at = (height(half, halves), span(j, count))
        return copy(part.at[at], near.at[at], s_a.at[0], r_a.at[unit], mate)

    def to_owner(j, count, half, halves, slot, rs, dev):
        h, p = height(half, halves), lax.rem(j, pq)
        return copy(pair.at[h, span(j, count)], far.at[slot, h, span(p, count)], s_b.at[0], rs, dev)

    def owner_sem(j, half, halves, slot):
        return r_b.at[slot, lax.rem(j, pq)] if halves == 1 else r_c.at[slot, lax.rem(j, pq) * halves + half]

    def whole(j):
        if paired:
            is_high, is_bent, is_mid = kinds(j)
            late = both(is_high, jnp.logical_not(fwd_all))
            late_own = both(away, jnp.logical_or(late, both(is_mid, jnp.logical_not(passes))))
            when(late_own, lambda: down_arrived(y, j))
            late_other = jnp.logical_or(jnp.logical_or(late, is_bent), both(is_mid, jnp.logical_not(fwd_mid)))
            when(late_other, lambda: down_arrived(other, j))
        else:
            for o in others:
                down_arrived(o, j)

    def ours(j):
        return lax.rem(j // pq, 2) == core

    def abroad(j):
        return both(ours(j), j // pq // 2 != x)

    def products(table, count, halves, lag, base):
        m = len(table) * halves

        def multiply(j, half):
            def wait():
                for i in range(count):
                    whole(j + i)

            when(half == 0, wait)
            h, at = height(half, halves), span(j, count)
            part[h, at] = jnp.dot(hidden[h, :], wd[:, at], preferred_element_type=jnp.float32).astype(jnp.bfloat16)

        def add(j, half, unit):
            h, at = height(half, halves), span(j, count)
            when(ours(j), lambda: to_mate(j, count, half, halves, unit).wait_recv())

            @pl.when(abroad(j))
            def _():
                pair[h, at] = (part[h, at].astype(jnp.float32) + near[h, at].astype(jnp.float32)).astype(jnp.bfloat16)

        def ship(j, half):
            owner = j // pq
            slot = lax.rem(x - owner // 2 + X, X) - 1
            to_owner(j, count, half, halves, slot, owner_sem(j, half, halves, slot), (f, owner)).start()

        def step(i):
            now, then = i < m, i >= lag
            i0, i1 = jnp.minimum(i, m - 1), jnp.maximum(i - lag, 0)
            j0, j1 = pick(table, i0 // halves), pick(table, i1 // halves)
            h0, h1 = lax.rem(i0, halves), lax.rem(i1, halves)

            def first_half():
                when(now, lambda: multiply(j0, h0))
                when(both(now, jnp.logical_not(ours(j0))), lambda: to_mate(j0, count, h0, halves, base + i).start())

            def second_half():
                when(then, lambda: add(j1, h1, base + i - lag))
                when(both(then, abroad(j1)), lambda: ship(j1, h1))

            if lag == 1:
                second_half()
                first_half()
            else:
                first_half()
                second_half()

        each(0, m + lag if m else 0, step)

    def finish(table, count, halves):
        def step(i):
            j, half = pick(table, i // halves), lax.rem(i, halves)

            @pl.when(j // pq == t)
            def _():
                h, at, to = height(half, halves), span(j, count), span(lax.rem(j, pq), count)
                acc = part[h, at].astype(jnp.float32) + near[h, at].astype(jnp.float32)
                for slot in range(X - 1):
                    to_owner(j, count, half, halves, slot, owner_sem(j, half, halves, slot), mate).wait_recv()
                    acc = acc + far[slot, h, to].astype(jnp.float32)
                mixed[h, to] = acc.astype(mixed.dtype)

        each(0, len(table) * halves, step)

    early, late_units = last_units[:-2], last_units[-2:]
    halves = 2 if n % 32 == 0 else 1
    products(pair_units, 2, 1, 2, 0)
    products(early, 1, 1, 1, len(pair_units))
    products(late_units, 1, halves, 2, len(pair_units) + len(early))
    finish(pair_units, 2, 1)
    finish(early, 1, 1)

    def gone(sem, ref):
        copy(ref, ref, sem, r_a.at[0], mate).wait_send()

    def gone_down(cond, sem, count):
        fold = next(c for c in range(1, Y + 1) if count % c == 0 and count // c <= nc)
        when(cond, lambda: gone(sem, wd.at[pl.ds(0, fold * rows_d), pl.ds(0, count // fold * W)]))

    when(away, lambda: gone(s_one.at[0], own_d))
    if paired:
        when(jnp.logical_or(guest_on[0], guest_on[1]), lambda: gone(s_tz.at[0], transit))
        when(guest_here, lambda: gone(s_tx.at[0], transit))
        for direction in range(2):
            gone_down(both(can(direction), near_ok(direction)), s_dz.at[direction], 2 * nc - pq)
            on = both(can(direction), jnp.logical_not(near_ok(direction)))
            gone_down(on, s_dz.at[direction], nc - pq + high[0])
        gone_down(at_home, s_dy.at[0], nc)
        gone_down(beyond, s_dy.at[0], nc - high[0])
        gone_down(both(away, jnp.logical_not(beyond)), s_dy.at[0], pq)
    else:
        for direction in range(2):
            gone_down(can(direction), s_dz.at[direction], nc)
        for i in range(Y - 1):
            gone_down(z >= 0, s_dy.at[i], nc)
    finish(late_units, 1, halves)
    gone(s_a.at[0], part.at[:, pl.ds(0, nc * W // 2)])
    gone(s_b.at[0], pair.at[:, pl.ds(0, (X - 1) * pq * W)])


def layer(mesh, gain, g, u, d, x):
    fs, T = mesh.shape["fs"], mesh.shape["tp"]
    Z, Y = lines(fs)
    X = T // 2
    rows, rows_d, n = g.shape[0], d.shape[0], x.shape[0]
    pq = d.shape[1] // W
    nc = T * pq
    nk = max(1, min(4, rows // 64))
    paired = Y == 2 and X == 2 and Z == T and pq % 2 == 0
    lanes = max(Y - 1, 1)
    dma = pltpu.SemaphoreType.DMA
    vmem, hbm = pl.BlockSpec(memory_space=pltpu.VMEM), pl.BlockSpec(memory_space=pltpu.HBM)
    bf = jnp.bfloat16
    return pl.pallas_call(
        functools.partial(layer_kernel, Z, Y, T, nk, paired),
        out_shape=(
            jax.ShapeDtypeStruct((rows * fs, g.shape[1]), bf),
            jax.ShapeDtypeStruct((rows * fs, g.shape[1]), bf),
            jax.ShapeDtypeStruct((rows_d * Y, d.shape[1] * T), bf),
            jax.ShapeDtypeStruct((n, d.shape[1]), bf),
        ),
        in_specs=[hbm] * 5,
        out_specs=[vmem] * 4,
        scratch_shapes=[
            pltpu.VMEM(gain.shape, jnp.float32),
            pltpu.VMEM(g.shape, jnp.float32), pltpu.VMEM(u.shape, jnp.float32), pltpu.VMEM(d.shape, jnp.float32),
            pltpu.VMEM(d.shape, bf), pltpu.VMEM(d.shape, bf), pltpu.VMEM(x.shape, bf), pltpu.VMEM((n, g.shape[1]), bf),
            pltpu.VMEM((n, nc * W), bf), pltpu.VMEM((n, nc * W), bf), pltpu.VMEM((n, nc * W), bf),
            pltpu.VMEM((max(X - 1, 1), n, pq * W), bf),
            dma((1,)), dma((nk,)), dma((nk,)), dma((1,)), dma((1,)),
            dma((1,)), dma((1,)), dma((lanes,)), dma((1,)), dma((Z, nk)), dma((fs,)),
            dma((1,)), dma((1,)), dma((1,)), dma((pq,)),
            dma((2,)), dma((lanes,)), dma((Y, nc)),
            dma((1,)), dma((sum(map(len, column_units(pq, nc, paired))) + 2,)), dma((1,)), dma((max(X - 1, 1), pq)),
            dma((max(X - 1, 1), 2 * pq)),
        ],
        compiler_params=pltpu.CompilerParams(
            collective_id=0, has_side_effects=True, vmem_limit_bytes=GRANT
        ),
        name="layer",
    )(*(pltpu.with_memory_space_constraint(v, pltpu.HBM) for v in (gain, g, u, d, x)))


def publish_kernel(cuts, wg, wu, wd, mixed, og, ou, od, om, sems):
    outs = []
    for a, (s, d) in enumerate(((wg, og), (wu, ou), (wd, od), (mixed, om))):
        h = s.shape[0] // cuts
        for i in range(cuts):
            outs.append(pltpu.make_async_copy(s.at[pl.ds(i * h, h), :], d.at[pl.ds(i * h, h), :], sems.at[a, i]))
    for c in outs:
        c.start()
    for c in outs:
        c.wait()


def publish(*arrays):
    vmem, any_ = pl.BlockSpec(memory_space=pltpu.VMEM), pl.BlockSpec(memory_space=pl.ANY)
    return pl.pallas_call(
        functools.partial(publish_kernel, CUTS),
        out_shape=tuple(jax.ShapeDtypeStruct(a.shape, a.dtype) for a in arrays),
        in_specs=[vmem] * 4,
        out_specs=[any_] * 4,
        scratch_shapes=[pltpu.SemaphoreType.DMA((4, CUTS))],
        compiler_params=pltpu.CompilerParams(vmem_limit_bytes=1024 * 1024),
        name="publish",
    )(*arrays)


def solution(mesh):
    def on_device(tokens, norm_gain, gate_weight, up_weight, down_weight):
        wg, wu, wd, mixed = layer(mesh, norm_gain[None, :], gate_weight, up_weight, down_weight, tokens)
        og, ou, od, om = publish(wg, wu, wd, mixed)
        return (om, og, ou, od)

    return jax.shard_map(
        on_device,
        mesh=mesh,
        in_specs=(P("fs", None), P("fs"), P("fs", "tp"), P("fs", "tp"), P("fs", "tp")),
        out_specs=(P("fs", "tp"), P(None, "tp"), P(None, "tp"), P("tp", None)),
        check_vma=False,
    )
```

```python
import functools

import jax
import jax.numpy as jnp
from jax import lax
from jax.experimental import pallas as pl
from jax.experimental.pallas import tpu as pltpu
from jax.sharding import PartitionSpec as P

MESH = pl.DeviceIdType.MESH
GRANT = 26 * 1024 * 1024
CUTS = 4
W = 128


def lines(fs):
    y = 1
    while 2 * (2 * y) * (2 * y) <= fs:
        y *= 2
    return fs // y, y


def when(cond, fn):
    pl.when(cond)(fn)


def each(lo, hi, fn):
    if hi > lo:
        pl.loop(lo, hi)(fn)


def layer_kernel(
    Z, Y, T, nk, paired,
    gain_hbm, g_hbm, u_hbm, d_hbm, x_hbm,
    wg, wu, wd, mixed,
    gain_row, stage_g, stage_u, stage_d, own_d, transit, normed, hidden, part, near, pair, far,
    in_gain, in_g, in_u, in_d, in_x, s_up, s_dn, s_y, s_det, r_w, r_o, s_one, s_tz, s_tx, r_t,
    s_dz, s_dy, r_d, s_a, r_a, s_b, r_b,
):
    f, t = lax.axis_index("fs"), lax.axis_index("tp")
    X = T // 2
    z, y = f // Y, lax.rem(f, Y)
    x, core = t // 2, lax.rem(t, 2)
    has_up, has_dn = z < Z - 1, z > 0
    up, dn = (f + Y, t), (f - Y, t)
    others = [lax.rem(y + i, Y) for i in range(1, Y)]
    across = [(z * Y + o, t) for o in others]
    rows = g_hbm.shape[0]
    ck = rows // nk
    rows_d, cols_d = d_hbm.shape
    pq = cols_d // W
    nc = T * pq
    n = x_hbm.shape[0]
    staged, full = (stage_g, stage_u), (wg, wu)
    pieces = [(k, a) for k in range(nk) for a in range(2)]

    def load(k, a):
        at = pl.ds(k * ck, ck)
        return pltpu.make_async_copy((g_hbm, u_hbm)[a].at[at, :], staged[a].at[at, :], (in_g, in_u)[a].at[k])

    load_d = pltpu.make_async_copy(d_hbm, stage_d, in_d.at[0])
    load_x = pltpu.make_async_copy(x_hbm, normed, in_x.at[0])
    load_gain = pltpu.make_async_copy(gain_hbm, gain_row, in_gain.at[0])
    load_gain.start()
    for k, a in pieces:
        load(k, a).start()
    load_d.start()
    load_x.start()

    barrier = pltpu.get_barrier_semaphore()

    def greet(dev):
        pl.semaphore_signal(barrier, inc=1, device_id=dev, device_id_type=MESH)

    when(has_up, lambda: greet(up))
    when(has_dn, lambda: greet(dn))
    for dev in across:
        greet(dev)
    for i in range(1, T):
        greet((f, lax.rem(t + i, T)))

    load_gain.wait()
    diagonal = lax.broadcasted_iota(jnp.int32, (rows, rows), 0) == lax.broadcasted_iota(jnp.int32, (rows, rows), 1)
    gain = jnp.sum(jnp.where(diagonal, jnp.broadcast_to(gain_row[...], (rows, rows)), 0.0), axis=1, keepdims=True)

    def copy(src, dst, ss, rs, dev):
        return pltpu.make_async_remote_copy(
            src_ref=src, dst_ref=dst, send_sem=ss, recv_sem=rs, device_id=dev, device_id_type=MESH
        )

    def weight(a, k, source, ss, rs, dev):
        at = full[a].at[pl.ds(pl.multiple_of(source * rows + k * ck, ck), ck), :]
        return copy(at, at, ss, rs, dev)

    def along(a, k, source, ss, dev):
        return weight(a, k, source, ss, r_w.at[source // Y, k], dev)

    def beyond_line(a, k, source, ss, dev):
        return weight(a, k, source, ss, r_o.at[source], dev)

    def taken(height, ss, rs):
        at = wg.at[pl.ds(0, height), :]
        return copy(at, at, ss, rs, (f, lax.rem(t + 1, T)))

    def arrived(k, source):
        taken(2 * ck, s_det.at[0], r_w.at[source // Y, k]).wait_recv()

    def arrived_whole(source):
        taken(2 * rows, s_det.at[0], r_o.at[source]).wait_recv()

    def start(cond, make):
        if cond is None:
            make().start()
        else:
            when(cond, lambda: make().start())

    def scale(k, a):
        load(k, a).wait()
        at = pl.ds(pl.multiple_of(f * rows + k * ck, ck), ck)
        full[a][at, :] = (gain[k * ck:(k + 1) * ck, :] * staged[a][pl.ds(k * ck, ck), :]).astype(jnp.bfloat16)

    def send_own(k, a):
        start(has_up, lambda: along(a, k, f, s_up.at[0], up))
        start(has_dn, lambda: along(a, k, f, s_dn.at[0], dn))
        for i in range(Y - 1):
            start(None, lambda i=i: beyond_line(a, k, f, s_y.at[i], across[i]))

    scale(*pieces[0])
    scale(*pieces[1])
    pl.semaphore_wait(barrier, Y + T - 2 + has_up.astype(jnp.int32) + has_dn.astype(jnp.int32))
    for i, piece in enumerate(pieces):
        if i + 2 < len(pieces):
            scale(*pieces[i + 2])
        send_own(*piece)

    def cols(j):
        return pl.ds(pl.multiple_of(j * W, W), W)

    def line_rows(line):
        return pl.ds(pl.multiple_of(line * rows_d, rows_d), rows_d)

    def down(line, j, ss, dev):
        at = wd.at[line_rows(line), cols(j)]
        return copy(at, at, ss, r_d.at[line, j], dev)

    def down_arrived(line, j):
        down(line, j, s_dy.at[0], (f, lax.rem(t + 1, T))).wait_recv()

    load_d.wait()
    own_d[...] = stage_d[...].astype(jnp.bfloat16)

    @pl.when(z == t)
    def _():
        wd[line_rows(y), pl.ds(pl.multiple_of(t * cols_d, cols_d), cols_d)] = stage_d[...].astype(jnp.bfloat16)

    def first(p):
        return copy(
            own_d.at[:, pl.ds(p * W, W)], wd.at[line_rows(y), cols(t * pq + p)],
            s_one.at[0], r_d.at[y, t * pq + p], (f, z),
        )

    load_x.wait()
    slab = 64 if n % 64 == 0 else n

    def normalise(i):
        at = pl.ds(pl.multiple_of(i * slab, slab), slab)
        v = normed[at, :].astype(jnp.float32)
        normed[at, :] = (v * lax.rsqrt(jnp.mean(v * v, axis=1, keepdims=True) + 1e-05)).astype(jnp.bfloat16)

    normalise(0)
    for p in range(pq):
        start(z != t, lambda p=p: first(p))
    each(1, n // slab, normalise)

    at_home = z == t
    can_up = jnp.logical_and(has_up, z >= t)
    can_dn = jnp.logical_and(has_dn, z <= t)
    inner = jnp.logical_and(has_up, has_dn)
    if paired:
        half = t // (T // 2)
        shift = (nc // 2) * (1 - half)
        far_up, far_dn = half == 0, half == 1
        beyond = jnp.logical_or(jnp.logical_and(z < t, far_dn), jnp.logical_and(z > t, far_up))
        fwd_mid = jnp.logical_or(
            jnp.logical_and(can_up, jnp.logical_not(far_up)), jnp.logical_and(can_dn, jnp.logical_not(far_dn))
        )
    fwd_all = jnp.logical_or(can_up, can_dn)
    if paired:
        passes = jnp.logical_or(fwd_all, beyond)
    away = jnp.logical_not(at_home)

    def column(r):
        return lax.rem(r + shift, nc)

    if paired:
        bent = (pq, lambda i: column(core * pq + i))
        low = (pq, lambda i: column((1 - core) * pq + i))
        mid = (pq // 2, lambda i: column((2 + core) * pq + i))
        high = (
            (pq, lambda i: column((3 - core) * pq + i)),
            (pq // 2, lambda i: column((2 + core) * pq + pq // 2 + i)),
        )
    else:
        mid = (nc, lambda i: i)
        high = ()
    high_count = sum(kind[0] for kind in high)

    def over(kind, fn):
        each(0, kind[0], lambda i: fn(kind[1](i)))

    def both(a, b):
        return jnp.logical_and(a, b)

    def kinds(j):
        r = lax.rem(j - shift + nc, nc)
        quarter = r // pq
        is_bent = quarter == core
        is_mid = jnp.logical_or(quarter == 1 - core, both(quarter == 2 + core, lax.rem(r, pq) < pq // 2))
        return jnp.logical_not(jnp.logical_or(is_bent, is_mid)), is_bent, is_mid

    def z_send(line, j, direction):
        return down(line, j, s_dz.at[direction], (up, dn)[direction])

    def near_ok(direction):
        return jnp.logical_not((far_up, far_dn)[direction])

    def can(direction):
        return (can_up, can_dn)[direction]

    def cross(j):
        for i in range(Y - 1):
            down(y, j, s_dy.at[i], across[i]).start()

    other = others[0]

    def assemble():
        for i in range(1, T):
            owner = lax.rem(t + i, T)
            for p in range(pq):
                down_arrived(y, owner * pq + p)
        for kind in high:
            over(kind, cross)
        if paired:
            @pl.when(inner)
            def _():
                over(low, cross)
                over(mid, cross)

    if paired:
        guest = lax.rem(t + T // 2, T)
        guest_dn = guest // (T // 2) == 1
        guest_here = jnp.logical_or(both(z < guest, guest_dn), both(z > guest, jnp.logical_not(guest_dn)))
        guest_on = (both(both(z >= guest, has_up), jnp.logical_not(guest_dn)), both(both(z <= guest, has_dn), guest_dn))

        def relay(p, direction, src):
            return copy(
                src.at[:, cols(p)], transit.at[:, cols(p)], s_tz.at[0], r_t.at[p], (up, dn)[direction]
            )

        def hand_over(p):
            return copy(
                transit.at[:, cols(p)], wd.at[line_rows(y), cols(t * pq + p)], s_tx.at[0], r_d.at[y, t * pq + p], (f, guest)
            )

    def leave(direction):
        if paired:
            @pl.when(both(z == guest, guest_on[direction]))
            def _():
                each(0, pq, lambda p: relay(p, direction, own_d).start())

        here = both(at_home, can(direction))
        if paired:
            here = both(here, jnp.logical_not(near_ok(direction)))

        @pl.when(here)
        def _():
            for kind in ((low, mid) if paired else (mid,)) + high:
                over(kind, lambda j: z_send(y, j, direction).start())

    def hook(s):
        when(z == s, lambda: leave(0))
        when(z == Z - 1 - s, lambda: leave(1))

    for step in range(1, Z):
        for k in range(nk):
            if step == 1 and k == nk // 2:
                when(at_home, assemble)
            for sign in (-1, 1):
                zs = z + sign * step
                source = zs * Y + y
                valid = zs >= 0 if sign < 0 else zs < Z
                onward = jnp.logical_and(valid, has_up if sign < 0 else has_dn)
                crossing = valid
                if paired and step == 1:
                    crossing = both(valid, zs != (0 if sign < 0 else Z - 1))
                when(valid, lambda k=k, s=source: arrived(k, s))
                for a in range(2):
                    if sign < 0:
                        start(onward, lambda a=a, k=k, s=source: along(a, k, s, s_up.at[0], up))
                    else:
                        start(onward, lambda a=a, k=k, s=source: along(a, k, s, s_dn.at[0], dn))
                    for i in range(Y - 1):
                        start(crossing, lambda a=a, k=k, s=source, i=i: beyond_line(a, k, s, s_y.at[i], across[i]))
        if step == 1:
            hook(0)
            if paired:
                ends = jnp.logical_not(inner)
                beside = across[0][0]
                when(ends, lambda: arrived_whole(beside))
                for k, a in pieces:
                    start(both(ends, has_up), lambda a=a, k=k: beyond_line(a, k, beside, s_det.at[0], up))
                    start(both(ends, has_dn), lambda a=a, k=k: beyond_line(a, k, beside, s_det.at[0], dn))
        hook(step)

    if paired:
        @pl.when(at_home)
        def _():
            @pl.when(jnp.logical_not(inner))
            def _():
                for kind in (bent, low, mid):
                    over(kind, cross)
            when(inner, lambda: over(bent, cross))

    else:
        when(at_home, lambda: over(mid, cross))

    if paired:
        @pl.when(guest_here)
        def _():
            def pass_on(p):
                copy(
                    transit.at[:, cols(p)], transit.at[:, cols(p)], s_tz.at[0], r_t.at[p], (f, guest)
                ).wait_recv()
                for direction in range(2):
                    when(guest_on[direction], lambda: relay(p, direction, transit).start())
                hand_over(p).start()
            each(0, pq, pass_on)

    if paired:
        @pl.when(both(at_home, inner))
        def _():
            def near_first(j):
                for direction in range(2):
                    when(near_ok(direction), lambda: z_send(y, j, direction).start())
            over(bent, near_first)

            def near_pair(is_high):
                def fn(j):
                    near_first(j)
                    down_arrived(other, j)
                    for direction in range(2):
                        toward = can(direction) if is_high else near_ok(direction)
                        when(toward, lambda: z_send(other, j, direction).start())
                return fn

            over(low, near_pair(False))
            for kind in high:
                over(kind, near_pair(True))
            over(mid, near_pair(False))

    @pl.when(away)
    def _():
        def bend(j):
            down_arrived(y, j)
            for direction in range(2):
                when(both(can(direction), near_ok(direction)), lambda: z_send(y, j, direction).start())
            cross(j)

        def straight(j):
            down_arrived(y, j)
            for direction in range(2):
                when(can(direction), lambda: z_send(y, j, direction).start())
            if paired:
                when(beyond, lambda: cross(j))
            else:
                cross(j)

        if paired:
            when(passes, lambda: over(low, straight))
            over(bent, bend)
            when(passes, lambda: over(mid, straight))
        else:
            over(mid, straight)

    if paired:
        @pl.when(both(fwd_mid, away))
        def _():
            def twin(j):
                down_arrived(other, j)
                for direction in range(2):
                    when(both(can(direction), near_ok(direction)), lambda: z_send(other, j, direction).start())
            over(low, twin)
            over(mid, twin)

        @pl.when(both(fwd_all, jnp.logical_or(away, jnp.logical_not(inner))))
        def _():
            def twins(j):
                @pl.when(away)
                def _():
                    down_arrived(y, j)
                    for direction in range(2):
                        when(can(direction), lambda: z_send(y, j, direction).start())
                down_arrived(other, j)
                for direction in range(2):
                    when(can(direction), lambda: z_send(other, j, direction).start())
            for kind in high:
                over(kind, twins)

    for zs in range(Z):
        for o in others:
            if paired and zs in (0, Z - 1):
                when(zs != z, lambda zs=zs, o=o: arrived_whole(zs * Y + o))
            else:
                arrived_whole(zs * Y + o)
    units = wg.shape[1]
    width = 256 if units % 256 == 0 else 128

    @pl.loop(0, units // width)
    def _(j):
        at = pl.ds(pl.multiple_of(j * width, width), width)
        gate = jnp.dot(normed[...], wg[:, at], preferred_element_type=jnp.float32)
        up_ = jnp.dot(normed[...], wu[:, at], preferred_element_type=jnp.float32)
        hidden[:, at] = (gate / (1.0 + jnp.exp(-gate)) * up_).astype(jnp.bfloat16)

    def drained(cond, shards, sem):
        when(cond, lambda: taken(2 * rows * shards, sem, r_w.at[0, 0]).wait_send())

    for q in range(Z - 1):
        drained(z == q, q + 1, s_up.at[0])
        drained(z == Z - 1 - q, q + 1, s_dn.at[0])
    for i in range(Y - 1):
        if paired:
            drained(inner, Z - 1, s_y.at[i])
            drained(jnp.logical_not(inner), Z, s_y.at[i])
        else:
            drained(z >= 0, Z, s_y.at[i])
    if paired:
        drained(jnp.logical_not(inner), 1, s_det.at[0])

    mate = (f, x * 2 + 1 - core)

    def span(j, count):
        return pl.ds(pl.multiple_of(j * W, W), count * W)

    grain = 2 if pq % 2 == 0 else 1

    def to_mate(j, count):
        at = span(j, count)
        return copy(part.at[:, at], near.at[:, at], s_a.at[0], r_a.at[j // grain], mate)

    def to_owner(j, slot, dev):
        p = lax.rem(j, pq)
        return copy(
            pair.at[:, span(j, grain)], far.at[slot, :, span(p, grain)], s_b.at[0], r_b.at[slot, p // grain], dev
        )

    def whole(j):
        if paired:
            is_high, is_bent, is_mid = kinds(j)
            late = both(is_high, jnp.logical_not(fwd_all))
            late_own = both(away, jnp.logical_or(late, both(is_mid, jnp.logical_not(passes))))
            when(late_own, lambda: down_arrived(y, j))
            late_other = jnp.logical_or(jnp.logical_or(late, is_bent), both(is_mid, jnp.logical_not(fwd_mid)))
            when(late_other, lambda: down_arrived(other, j))
        else:
            for o in others:
                down_arrived(o, j)

    def ours(j):
        return lax.rem(j // pq, 2) == core

    def multiply(j, count):
        for i in range(count):
            whole(j + i)
        at = span(j, count)
        part[:, at] = jnp.dot(hidden[...], wd[:, at], preferred_element_type=jnp.float32).astype(jnp.bfloat16)
        when(jnp.logical_not(ours(j)), lambda: to_mate(j, count).start())

    def pass_sum(j):
        owner, at = j // pq, span(j, grain)
        to_mate(j, grain).wait_recv()
        pair[:, at] = (part[:, at].astype(jnp.float32) + near[:, at].astype(jnp.float32)).astype(jnp.bfloat16)
        to_owner(j, lax.rem(x - owner // 2 + X, X) - 1, (f, owner)).start()

    def sums_arrived(j):
        to_mate(j, grain).wait_recv()
        for slot in range(X - 1):
            to_owner(j, slot, mate).wait_recv()

    def finish(j, count):
        at, to = span(j, count), span(lax.rem(j, pq), count)
        acc = part[:, at].astype(jnp.float32) + near[:, at].astype(jnp.float32)
        for slot in range(X - 1):
            acc = acc + far[slot, :, to].astype(jnp.float32)
        mixed[:, to] = acc.astype(mixed.dtype)

    if paired:
        upper = (z >= Z // 2).astype(jnp.int32)
        is_far = half == 1 - upper
        is_edge = jnp.logical_or(t == 0, t == T - 1)
        block_a, block_b, block_c, block_d = core * pq, (1 - core) * pq, (2 + core) * pq, (3 - core) * pq
        orders = (
            (block_b, block_d, block_b + 2, block_a, block_d + 2, block_a + 2,
             block_c + 2, block_c, block_c + 3, block_c + 1),
            (block_c, block_c + 2, block_b, block_b + 2, block_a + 2, block_d,
             block_d + 2, block_d + 3, block_a, block_a + 1),
            (block_c, block_d, block_d + 2, block_c + 2, block_b, block_b + 2,
             block_a + 2, block_a + 3, block_a, block_a + 1),
        )
        turn = upper * (nc // 2)
        chosen = [
            lax.rem(jnp.where(is_far, v, jnp.where(is_edge, e, i)) + turn, nc) for v, e, i in zip(*orders)
        ]
        doubles, singles = chosen[:6], chosen[6:]

        def pick(table, i):
            return sum(v * (i == e).astype(jnp.int32) for e, v in enumerate(table))

        over_there = lax.rem(t + T // 2, T) * pq
        first_at = jnp.where(is_far, 3, jnp.where(is_edge, 0, 5))
        second_at = jnp.where(is_far, 5, jnp.where(is_edge, 1, 6))

        def double(i):
            multiply(pick(doubles, i), grain)
            second = i == second_at
            when(jnp.logical_or(i == first_at, second), lambda: pass_sum(over_there + second.astype(jnp.int32) * grain))

        def single(i):
            multiply(pick(singles, i), 1)
            when(both(i == 0, second_at == 6), lambda: pass_sum(over_there + grain))

        each(0, len(doubles), double)
        each(0, len(singles) - 1, single)
        each(0, pq // grain, lambda i: sums_arrived(t * pq + i * grain))
        finish(t * pq + 2, 2)
        finish(t * pq, 1)
        multiply(singles[-1], 1)
        finish(t * pq + 1, 1)
    else:
        each(0, nc // grain, lambda i: multiply(i * grain, grain))
        for i in range(1, X):
            base = (lax.rem(x + i, X) * 2 + core) * pq
            each(0, pq // grain, lambda i, base=base: pass_sum(base + i * grain))
        each(0, pq // grain, lambda i: sums_arrived(t * pq + i * grain))
        each(0, pq // grain, lambda i: finish(t * pq + i * grain, grain))

    def gone(sem, ref):
        copy(ref, ref, sem, r_a.at[0], mate).wait_send()

    def gone_down(cond, sem, count):
        fold = next(c for c in range(1, Y + 1) if count % c == 0 and count // c <= nc)
        when(cond, lambda: gone(sem, wd.at[pl.ds(0, fold * rows_d), pl.ds(0, count // fold * W)]))

    when(away, lambda: gone(s_one.at[0], own_d))
    if paired:
        when(jnp.logical_or(guest_on[0], guest_on[1]), lambda: gone(s_tz.at[0], transit))
        when(guest_here, lambda: gone(s_tx.at[0], transit))
        for direction in range(2):
            gone_down(both(can(direction), near_ok(direction)), s_dz.at[direction], 2 * nc - pq)
            on = both(can(direction), jnp.logical_not(near_ok(direction)))
            gone_down(on, s_dz.at[direction], nc - pq + high_count)
        gone_down(at_home, s_dy.at[0], nc)
        gone_down(beyond, s_dy.at[0], nc - high_count)
        gone_down(both(away, jnp.logical_not(beyond)), s_dy.at[0], pq)
    else:
        for direction in range(2):
            gone_down(can(direction), s_dz.at[direction], nc)
        for i in range(Y - 1):
            gone_down(z >= 0, s_dy.at[i], nc)
    gone(s_a.at[0], part.at[:, pl.ds(0, nc * W // 2)])
    gone(s_b.at[0], pair.at[:, pl.ds(0, (X - 1) * pq * W)])


def layer(mesh, gain, g, u, d, x):
    fs, T = mesh.shape["fs"], mesh.shape["tp"]
    Z, Y = lines(fs)
    X = T // 2
    rows, rows_d, n = g.shape[0], d.shape[0], x.shape[0]
    pq = d.shape[1] // W
    nc = T * pq
    nk = max(1, min(4, rows // 64))
    paired = Y == 2 and X == 2 and Z == T and pq == 4
    grain = 2 if pq % 2 == 0 else 1
    lanes = max(Y - 1, 1)
    dma = pltpu.SemaphoreType.DMA
    vmem, hbm = pl.BlockSpec(memory_space=pltpu.VMEM), pl.BlockSpec(memory_space=pltpu.HBM)
    bf = jnp.bfloat16
    return pl.pallas_call(
        functools.partial(layer_kernel, Z, Y, T, nk, paired),
        out_shape=(
            jax.ShapeDtypeStruct((rows * fs, g.shape[1]), bf),
            jax.ShapeDtypeStruct((rows * fs, g.shape[1]), bf),
            jax.ShapeDtypeStruct((rows_d * Y, d.shape[1] * T), bf),
            jax.ShapeDtypeStruct((n, d.shape[1]), bf),
        ),
        in_specs=[hbm] * 5,
        out_specs=[vmem] * 4,
        scratch_shapes=[
            pltpu.VMEM(gain.shape, jnp.float32),
            pltpu.VMEM(g.shape, jnp.float32), pltpu.VMEM(u.shape, jnp.float32), pltpu.VMEM(d.shape, jnp.float32),
            pltpu.VMEM(d.shape, bf), pltpu.VMEM(d.shape, bf), pltpu.VMEM(x.shape, bf), pltpu.VMEM((n, g.shape[1]), bf),
            pltpu.VMEM((n, nc * W), bf), pltpu.VMEM((n, nc * W), bf), pltpu.VMEM((n, nc * W), bf),
            pltpu.VMEM((max(X - 1, 1), n, pq * W), bf),
            dma((1,)), dma((nk,)), dma((nk,)), dma((1,)), dma((1,)),
            dma((1,)), dma((1,)), dma((lanes,)), dma((1,)), dma((Z, nk)), dma((fs,)),
            dma((1,)), dma((1,)), dma((1,)), dma((pq,)),
            dma((2,)), dma((lanes,)), dma((Y, nc)),
            dma((1,)), dma((nc // grain,)), dma((1,)), dma((max(X - 1, 1), pq // grain)),
        ],
        compiler_params=pltpu.CompilerParams(
            collective_id=0, has_side_effects=True, vmem_limit_bytes=GRANT
        ),
        name="layer",
    )(*(pltpu.with_memory_space_constraint(v, pltpu.HBM) for v in (gain, g, u, d, x)))


def publish_kernel(cuts, wg, wu, wd, mixed, og, ou, od, om, sems):
    outs = []
    for a, (s, d) in enumerate(((wg, og), (wu, ou), (wd, od), (mixed, om))):
        h = s.shape[0] // cuts
        for i in range(cuts):
            outs.append(pltpu.make_async_copy(s.at[pl.ds(i * h, h), :], d.at[pl.ds(i * h, h), :], sems.at[a, i]))
    for c in outs:
        c.start()
    for c in outs:
        c.wait()


def publish(*arrays):
    vmem, any_ = pl.BlockSpec(memory_space=pltpu.VMEM), pl.BlockSpec(memory_space=pl.ANY)
    return pl.pallas_call(
        functools.partial(publish_kernel, CUTS),
        out_shape=tuple(jax.ShapeDtypeStruct(a.shape, a.dtype) for a in arrays),
        in_specs=[vmem] * 4,
        out_specs=[any_] * 4,
        scratch_shapes=[pltpu.SemaphoreType.DMA((4, CUTS))],
        compiler_params=pltpu.CompilerParams(vmem_limit_bytes=1024 * 1024),
        name="publish",
    )(*arrays)


def solution(mesh):
    def on_device(tokens, norm_gain, gate_weight, up_weight, down_weight):
        wg, wu, wd, mixed = layer(mesh, norm_gain[None, :], gate_weight, up_weight, down_weight, tokens)
        og, ou, od, om = publish(wg, wu, wd, mixed)
        return (om, og, ou, od)

    return jax.shard_map(
        on_device,
        mesh=mesh,
        in_specs=(P("fs", None), P("fs"), P("fs", "tp"), P("fs", "tp"), P("fs", "tp")),
        out_specs=(P("fs", "tp"), P(None, "tp"), P(None, "tp"), P("tp", None)),
        check_vma=False,
    )
```

```python
import functools

import jax
import jax.numpy as jnp
from jax import lax
from jax.experimental import pallas as pl
from jax.experimental.pallas import tpu as pltpu
from jax.sharding import PartitionSpec as P

MESH = pl.DeviceIdType.MESH
GRANT = 26 * 1024 * 1024
CUTS = 4
W = 128


def lines(fs):
    y = 1
    while 2 * (2 * y) * (2 * y) <= fs:
        y *= 2
    return fs // y, y


def when(cond, fn):
    pl.when(cond)(fn)


def each(lo, hi, fn):
    if hi > lo:
        pl.loop(lo, hi)(fn)


def layer_kernel(
    Z, Y, T, nk, paired,
    gain_hbm, g_hbm, u_hbm, d_hbm, x_hbm,
    wg, wu, wd, mixed,
    gain_row, stage_g, stage_u, stage_d, own_d, transit, normed, hidden, part, near, pair, far,
    in_gain, in_g, in_u, in_d, in_x, s_up, s_dn, s_y, s_det, r_w, r_o, s_one, s_tz, s_tx, r_t,
    s_dz, s_dy, r_d, s_a, r_a, s_b, r_b,
):
    f, t = lax.axis_index("fs"), lax.axis_index("tp")
    X = T // 2
    z, y = f // Y, lax.rem(f, Y)
    x, core = t // 2, lax.rem(t, 2)
    has_up, has_dn = z < Z - 1, z > 0
    up, dn = (f + Y, t), (f - Y, t)
    others = [lax.rem(y + i, Y) for i in range(1, Y)]
    across = [(z * Y + o, t) for o in others]
    rows = g_hbm.shape[0]
    ck = rows // nk
    rows_d, cols_d = d_hbm.shape
    pq = cols_d // W
    nc = T * pq
    n = x_hbm.shape[0]
    staged, full = (stage_g, stage_u), (wg, wu)
    pieces = [(k, a) for k in range(nk) for a in range(2)]

    def load(k, a):
        at = pl.ds(k * ck, ck)
        return pltpu.make_async_copy((g_hbm, u_hbm)[a].at[at, :], staged[a].at[at, :], (in_g, in_u)[a].at[k])

    load_d = pltpu.make_async_copy(d_hbm, stage_d, in_d.at[0])
    load_x = pltpu.make_async_copy(x_hbm, normed, in_x.at[0])
    load_gain = pltpu.make_async_copy(gain_hbm, gain_row, in_gain.at[0])
    load_gain.start()
    for k, a in pieces:
        load(k, a).start()
    load_d.start()
    load_x.start()

    barrier = pltpu.get_barrier_semaphore()

    def greet(dev):
        pl.semaphore_signal(barrier, inc=1, device_id=dev, device_id_type=MESH)

    when(has_up, lambda: greet(up))
    when(has_dn, lambda: greet(dn))
    for dev in across:
        greet(dev)
    for i in range(1, T):
        greet((f, lax.rem(t + i, T)))

    load_gain.wait()
    diagonal = lax.broadcasted_iota(jnp.int32, (rows, rows), 0) == lax.broadcasted_iota(jnp.int32, (rows, rows), 1)
    gain = jnp.sum(jnp.where(diagonal, jnp.broadcast_to(gain_row[...], (rows, rows)), 0.0), axis=1, keepdims=True)

    def copy(src, dst, ss, rs, dev):
        return pltpu.make_async_remote_copy(
            src_ref=src, dst_ref=dst, send_sem=ss, recv_sem=rs, device_id=dev, device_id_type=MESH
        )

    def weight(a, k, source, ss, rs, dev):
        at = full[a].at[pl.ds(pl.multiple_of(source * rows + k * ck, ck), ck), :]
        return copy(at, at, ss, rs, dev)

    def along(a, k, source, ss, dev):
        return weight(a, k, source, ss, r_w.at[source // Y, k], dev)

    def beyond_line(a, k, source, ss, dev):
        return weight(a, k, source, ss, r_o.at[source], dev)

    def taken(height, ss, rs):
        at = wg.at[pl.ds(0, height), :]
        return copy(at, at, ss, rs, (f, lax.rem(t + 1, T)))

    def arrived(k, source):
        taken(2 * ck, s_det.at[0], r_w.at[source // Y, k]).wait_recv()

    def arrived_whole(source):
        taken(2 * rows, s_det.at[0], r_o.at[source]).wait_recv()

    def start(cond, make):
        if cond is None:
            make().start()
        else:
            when(cond, lambda: make().start())

    def scale(k, a):
        load(k, a).wait()
        at = pl.ds(pl.multiple_of(f * rows + k * ck, ck), ck)
        full[a][at, :] = (gain[k * ck:(k + 1) * ck, :] * staged[a][pl.ds(k * ck, ck), :]).astype(jnp.bfloat16)

    def send_own(k, a):
        start(has_up, lambda: along(a, k, f, s_up.at[0], up))
        start(has_dn, lambda: along(a, k, f, s_dn.at[0], dn))
        for i in range(Y - 1):
            start(None, lambda i=i: beyond_line(a, k, f, s_y.at[i], across[i]))

    scale(*pieces[0])
    scale(*pieces[1])
    pl.semaphore_wait(barrier, Y + T - 2 + has_up.astype(jnp.int32) + has_dn.astype(jnp.int32))
    for i, piece in enumerate(pieces):
        if i + 2 < len(pieces):
            scale(*pieces[i + 2])
        send_own(*piece)

    def cols(j):
        return pl.ds(pl.multiple_of(j * W, W), W)

    def line_rows(line):
        return pl.ds(pl.multiple_of(line * rows_d, rows_d), rows_d)

    def down(line, j, ss, dev):
        at = wd.at[line_rows(line), cols(j)]
        return copy(at, at, ss, r_d.at[line, j], dev)

    def down_arrived(line, j):
        down(line, j, s_dy.at[0], (f, lax.rem(t + 1, T))).wait_recv()

    load_d.wait()
    own_d[...] = stage_d[...].astype(jnp.bfloat16)

    @pl.when(z == t)
    def _():
        wd[line_rows(y), pl.ds(pl.multiple_of(t * cols_d, cols_d), cols_d)] = stage_d[...].astype(jnp.bfloat16)

    def first(p):
        return copy(
            own_d.at[:, pl.ds(p * W, W)], wd.at[line_rows(y), cols(t * pq + p)],
            s_one.at[0], r_d.at[y, t * pq + p], (f, z),
        )

    load_x.wait()
    slab = 64 if n % 64 == 0 else n

    def normalise(i):
        at = pl.ds(pl.multiple_of(i * slab, slab), slab)
        v = normed[at, :].astype(jnp.float32)
        normed[at, :] = (v * lax.rsqrt(jnp.mean(v * v, axis=1, keepdims=True) + 1e-05)).astype(jnp.bfloat16)

    normalise(0)
    for p in range(pq):
        start(z != t, lambda p=p: first(p))
    each(1, n // slab, normalise)

    at_home = z == t
    can_up = jnp.logical_and(has_up, z >= t)
    can_dn = jnp.logical_and(has_dn, z <= t)
    inner = jnp.logical_and(has_up, has_dn)
    if paired:
        half = t // (T // 2)
        shift = (nc // 2) * (1 - half)
        far_up, far_dn = half == 0, half == 1
        beyond = jnp.logical_or(jnp.logical_and(z < t, far_dn), jnp.logical_and(z > t, far_up))
        fwd_mid = jnp.logical_or(
            jnp.logical_and(can_up, jnp.logical_not(far_up)), jnp.logical_and(can_dn, jnp.logical_not(far_dn))
        )
    fwd_all = jnp.logical_or(can_up, can_dn)
    if paired:
        passes = jnp.logical_or(fwd_all, beyond)
    away = jnp.logical_not(at_home)

    def column(r):
        return lax.rem(r + shift, nc)

    if paired:
        bent = (pq, lambda i: column(core * pq + i))
        low = (pq, lambda i: column((1 - core) * pq + i))
        mid = (pq // 2, lambda i: column((2 + core) * pq + i))
        high = (
            (pq, lambda i: column((3 - core) * pq + i)),
            (pq // 2, lambda i: column((2 + core) * pq + pq // 2 + i)),
        )
    else:
        mid = (nc, lambda i: i)
        high = ()
    high_count = sum(kind[0] for kind in high)

    def over(kind, fn):
        each(0, kind[0], lambda i: fn(kind[1](i)))

    def both(a, b):
        return jnp.logical_and(a, b)

    def kinds(j):
        r = lax.rem(j - shift + nc, nc)
        quarter = r // pq
        is_bent = quarter == core
        is_mid = jnp.logical_or(quarter == 1 - core, both(quarter == 2 + core, lax.rem(r, pq) < pq // 2))
        return jnp.logical_not(jnp.logical_or(is_bent, is_mid)), is_bent, is_mid

    def z_send(line, j, direction):
        return down(line, j, s_dz.at[direction], (up, dn)[direction])

    def near_ok(direction):
        return jnp.logical_not((far_up, far_dn)[direction])

    def can(direction):
        return (can_up, can_dn)[direction]

    def cross(j):
        for i in range(Y - 1):
            down(y, j, s_dy.at[i], across[i]).start()

    other = others[0]

    def assemble():
        for i in range(1, T):
            owner = lax.rem(t + i, T)
            for p in range(pq):
                down_arrived(y, owner * pq + p)
        for kind in high:
            over(kind, cross)
        if paired:
            @pl.when(inner)
            def _():
                over(low, cross)
                over(mid, cross)

    if paired:
        guest = lax.rem(t + T // 2, T)
        guest_dn = guest // (T // 2) == 1
        guest_here = jnp.logical_or(both(z < guest, guest_dn), both(z > guest, jnp.logical_not(guest_dn)))
        guest_on = (both(both(z >= guest, has_up), jnp.logical_not(guest_dn)), both(both(z <= guest, has_dn), guest_dn))

        def relay(p, direction, src):
            return copy(
                src.at[:, cols(p)], transit.at[:, cols(p)], s_tz.at[0], r_t.at[p], (up, dn)[direction]
            )

        def hand_over(p):
            return copy(
                transit.at[:, cols(p)], wd.at[line_rows(y), cols(t * pq + p)], s_tx.at[0], r_d.at[y, t * pq + p], (f, guest)
            )

    def leave(direction):
        if paired:
            @pl.when(both(z == guest, guest_on[direction]))
            def _():
                each(0, pq, lambda p: relay(p, direction, own_d).start())

        here = both(at_home, can(direction))
        if paired:
            here = both(here, jnp.logical_not(near_ok(direction)))

        @pl.when(here)
        def _():
            for kind in ((low, mid) if paired else (mid,)) + high:
                over(kind, lambda j: z_send(y, j, direction).start())

    def hook(s):
        when(z == s, lambda: leave(0))
        when(z == Z - 1 - s, lambda: leave(1))

    for step in range(1, Z):
        for k in range(nk):
            if step == 1 and k == nk // 2:
                when(at_home, assemble)
            for sign in (-1, 1):
                zs = z + sign * step
                source = zs * Y + y
                valid = zs >= 0 if sign < 0 else zs < Z
                onward = jnp.logical_and(valid, has_up if sign < 0 else has_dn)
                crossing = valid
                if paired and step == 1:
                    crossing = both(valid, zs != (0 if sign < 0 else Z - 1))
                when(valid, lambda k=k, s=source: arrived(k, s))
                for a in range(2):
                    if sign < 0:
                        start(onward, lambda a=a, k=k, s=source: along(a, k, s, s_up.at[0], up))
                    else:
                        start(onward, lambda a=a, k=k, s=source: along(a, k, s, s_dn.at[0], dn))
                    for i in range(Y - 1):
                        start(crossing, lambda a=a, k=k, s=source, i=i: beyond_line(a, k, s, s_y.at[i], across[i]))
        if step == 1:
            hook(0)
            if paired:
                ends = jnp.logical_not(inner)
                beside = across[0][0]
                when(ends, lambda: arrived_whole(beside))
                for k, a in pieces:
                    start(both(ends, has_up), lambda a=a, k=k: beyond_line(a, k, beside, s_det.at[0], up))
                    start(both(ends, has_dn), lambda a=a, k=k: beyond_line(a, k, beside, s_det.at[0], dn))
        hook(step)

    if paired:
        @pl.when(at_home)
        def _():
            @pl.when(jnp.logical_not(inner))
            def _():
                for kind in (bent, low, mid):
                    over(kind, cross)
            when(inner, lambda: over(bent, cross))

    else:
        when(at_home, lambda: over(mid, cross))

    if paired:
        @pl.when(guest_here)
        def _():
            def pass_on(p):
                copy(
                    transit.at[:, cols(p)], transit.at[:, cols(p)], s_tz.at[0], r_t.at[p], (f, guest)
                ).wait_recv()
                for direction in range(2):
                    when(guest_on[direction], lambda: relay(p, direction, transit).start())
                hand_over(p).start()
            each(0, pq, pass_on)

    if paired:
        @pl.when(both(at_home, inner))
        def _():
            def near_first(j):
                for direction in range(2):
                    when(near_ok(direction), lambda: z_send(y, j, direction).start())
            over(bent, near_first)

            def near_pair(is_high):
                def fn(j):
                    near_first(j)
                    down_arrived(other, j)
                    for direction in range(2):
                        toward = can(direction) if is_high else near_ok(direction)
                        when(toward, lambda: z_send(other, j, direction).start())
                return fn

            over(low, near_pair(False))
            for kind in high:
                over(kind, near_pair(True))
            over(mid, near_pair(False))

    @pl.when(away)
    def _():
        def bend(j):
            down_arrived(y, j)
            for direction in range(2):
                when(both(can(direction), near_ok(direction)), lambda: z_send(y, j, direction).start())
            cross(j)

        def straight(j):
            down_arrived(y, j)
            for direction in range(2):
                when(can(direction), lambda: z_send(y, j, direction).start())
            if paired:
                when(beyond, lambda: cross(j))
            else:
                cross(j)

        if paired:
            when(passes, lambda: over(low, straight))
            over(bent, bend)
            when(passes, lambda: over(mid, straight))
        else:
            over(mid, straight)

    if paired:
        @pl.when(both(fwd_mid, away))
        def _():
            def twin(j):
                down_arrived(other, j)
                for direction in range(2):
                    when(both(can(direction), near_ok(direction)), lambda: z_send(other, j, direction).start())
            over(low, twin)
            over(mid, twin)

        @pl.when(both(fwd_all, jnp.logical_or(away, jnp.logical_not(inner))))
        def _():
            def twins(j):
                @pl.when(away)
                def _():
                    down_arrived(y, j)
                    for direction in range(2):
                        when(can(direction), lambda: z_send(y, j, direction).start())
                down_arrived(other, j)
                for direction in range(2):
                    when(can(direction), lambda: z_send(other, j, direction).start())
            for kind in high:
                over(kind, twins)

    for zs in range(Z):
        for o in others:
            if paired and zs in (0, Z - 1):
                when(zs != z, lambda zs=zs, o=o: arrived_whole(zs * Y + o))
            else:
                arrived_whole(zs * Y + o)
    units = wg.shape[1]
    width = 256 if units % 256 == 0 else 128

    @pl.loop(0, units // width)
    def _(j):
        at = pl.ds(pl.multiple_of(j * width, width), width)
        gate = jnp.dot(normed[...], wg[:, at], preferred_element_type=jnp.float32)
        up_ = jnp.dot(normed[...], wu[:, at], preferred_element_type=jnp.float32)
        hidden[:, at] = (gate / (1.0 + jnp.exp(-gate)) * up_).astype(jnp.bfloat16)

    def drained(cond, shards, sem):
        when(cond, lambda: taken(2 * rows * shards, sem, r_w.at[0, 0]).wait_send())

    for q in range(Z - 1):
        drained(z == q, q + 1, s_up.at[0])
        drained(z == Z - 1 - q, q + 1, s_dn.at[0])
    for i in range(Y - 1):
        if paired:
            drained(inner, Z - 1, s_y.at[i])
            drained(jnp.logical_not(inner), Z, s_y.at[i])
        else:
            drained(z >= 0, Z, s_y.at[i])
    if paired:
        drained(jnp.logical_not(inner), 1, s_det.at[0])

    mate = (f, x * 2 + 1 - core)

    def span(j, count):
        return pl.ds(pl.multiple_of(j * W, W), count * W)

    grain = 2 if pq % 2 == 0 else 1

    def to_mate(j, count):
        at, lone = span(j, count), j // grain
        if count < grain:
            odd = lax.rem(j, grain)
            lone = odd * (nc // grain) + (1 - odd) * lone
        return copy(part.at[:, at], near.at[:, at], s_a.at[0], r_a.at[lone], mate)

    def to_owner(j, count, slot, dev):
        p = lax.rem(j, pq)
        return copy(
            pair.at[:, span(j, count)], far.at[slot, :, span(p, count)], s_b.at[0], r_b.at[slot, p // grain], dev
        )

    def whole(j):
        if paired:
            is_high, is_bent, is_mid = kinds(j)
            late = both(is_high, jnp.logical_not(fwd_all))
            late_own = both(away, jnp.logical_or(late, both(is_mid, jnp.logical_not(passes))))
            when(late_own, lambda: down_arrived(y, j))
            late_other = jnp.logical_or(jnp.logical_or(late, is_bent), both(is_mid, jnp.logical_not(fwd_mid)))
            when(late_other, lambda: down_arrived(other, j))
        else:
            for o in others:
                down_arrived(o, j)

    def ours(j):
        return lax.rem(j // pq, 2) == core

    def multiply(j, count):
        for i in range(count):
            whole(j + i)
        at = span(j, count)
        part[:, at] = jnp.dot(hidden[...], wd[:, at], preferred_element_type=jnp.float32).astype(jnp.bfloat16)
        when(jnp.logical_not(ours(j)), lambda: to_mate(j, count).start())

    def pass_sum(j, count):
        owner, at = j // pq, span(j, count)
        to_mate(j, count).wait_recv()
        pair[:, at] = (part[:, at].astype(jnp.float32) + near[:, at].astype(jnp.float32)).astype(jnp.bfloat16)
        to_owner(j, count, lax.rem(x - owner // 2 + X, X) - 1, (f, owner)).start()

    def sums_arrived(j):
        to_mate(j, grain).wait_recv()
        for slot in range(X - 1):
            to_owner(j, grain, slot, mate).wait_recv()

    def finish(j, count):
        at, to = span(j, count), span(lax.rem(j, pq), count)
        acc = part[:, at].astype(jnp.float32) + near[:, at].astype(jnp.float32)
        for slot in range(X - 1):
            acc = acc + far[slot, :, to].astype(jnp.float32)
        mixed[:, to] = acc.astype(mixed.dtype)

    if paired:
        upper = (z >= Z // 2).astype(jnp.int32)
        is_far = half == 1 - upper
        is_edge = jnp.logical_or(t == 0, t == T - 1)
        block_a, block_b, block_c, block_d = core * pq, (1 - core) * pq, (2 + core) * pq, (3 - core) * pq
        orders = (
            (block_b, block_d, block_b + 2, block_a, block_d + 2, block_a + 2,
             block_c + 2, block_c, block_c + 3, block_c + 1),
            (block_c, block_c + 2, block_b, block_b + 2, block_a + 2, block_d,
             block_d + 2, block_d + 3, block_a, block_a + 1),
            (block_c, block_d, block_d + 2, block_c + 2, block_b, block_b + 2,
             block_a + 2, block_a + 3, block_a, block_a + 1),
        )
        turn = upper * (nc // 2)
        chosen = [
            lax.rem(jnp.where(is_far, v, jnp.where(is_edge, e, i)) + turn, nc) for v, e, i in zip(*orders)
        ]
        doubles, singles = chosen[:6], chosen[6:]

        def pick(table, i):
            return sum(v * (i == e).astype(jnp.int32) for e, v in enumerate(table))

        over_there = lax.rem(t + T // 2, T) * pq
        first_at = jnp.where(is_far, 3, jnp.where(is_edge, 0, 5))
        second_at = jnp.where(is_far, 5, jnp.where(is_edge, 1, 6))

        def double(i):
            multiply(pick(doubles, i), grain)
            second = i == second_at
            when(jnp.logical_or(i == first_at, second), lambda: pass_sum(over_there + second.astype(jnp.int32) * grain, grain))

        def single(i):
            multiply(pick(singles, i), 1)
            when(both(i < grain, second_at == 6), lambda: pass_sum(over_there + grain + i, 1))

        each(0, len(doubles), double)
        each(0, len(singles) - 1, single)
        each(0, pq // grain, lambda i: sums_arrived(t * pq + i * grain))
        finish(t * pq + 2, 2)
        finish(t * pq, 1)
        multiply(singles[-1], 1)
        finish(t * pq + 1, 1)
    else:
        each(0, nc // grain, lambda i: multiply(i * grain, grain))
        for i in range(1, X):
            base = (lax.rem(x + i, X) * 2 + core) * pq
            each(0, pq // grain, lambda i, base=base: pass_sum(base + i * grain, grain))
        each(0, pq // grain, lambda i: sums_arrived(t * pq + i * grain))
        each(0, pq // grain, lambda i: finish(t * pq + i * grain, grain))

    def gone(sem, ref):
        copy(ref, ref, sem, r_a.at[0], mate).wait_send()

    def gone_down(cond, sem, count):
        fold = next(c for c in range(1, Y + 1) if count % c == 0 and count // c <= nc)
        when(cond, lambda: gone(sem, wd.at[pl.ds(0, fold * rows_d), pl.ds(0, count // fold * W)]))

    when(away, lambda: gone(s_one.at[0], own_d))
    if paired:
        when(jnp.logical_or(guest_on[0], guest_on[1]), lambda: gone(s_tz.at[0], transit))
        when(guest_here, lambda: gone(s_tx.at[0], transit))
        for direction in range(2):
            gone_down(both(can(direction), near_ok(direction)), s_dz.at[direction], 2 * nc - pq)
            on = both(can(direction), jnp.logical_not(near_ok(direction)))
            gone_down(on, s_dz.at[direction], nc - pq + high_count)
        gone_down(at_home, s_dy.at[0], nc)
        gone_down(beyond, s_dy.at[0], nc - high_count)
        gone_down(both(away, jnp.logical_not(beyond)), s_dy.at[0], pq)
    else:
        for direction in range(2):
            gone_down(can(direction), s_dz.at[direction], nc)
        for i in range(Y - 1):
            gone_down(z >= 0, s_dy.at[i], nc)
    gone(s_a.at[0], part.at[:, pl.ds(0, nc * W // 2)])
    gone(s_b.at[0], pair.at[:, pl.ds(0, (X - 1) * pq * W)])


def layer(mesh, gain, g, u, d, x):
    fs, T = mesh.shape["fs"], mesh.shape["tp"]
    Z, Y = lines(fs)
    X = T // 2
    rows, rows_d, n = g.shape[0], d.shape[0], x.shape[0]
    pq = d.shape[1] // W
    nc = T * pq
    nk = max(1, min(4, rows // 64))
    paired = Y == 2 and X == 2 and Z == T and pq == 4
    grain = 2 if pq % 2 == 0 else 1
    lanes = max(Y - 1, 1)
    dma = pltpu.SemaphoreType.DMA
    vmem, hbm = pl.BlockSpec(memory_space=pltpu.VMEM), pl.BlockSpec(memory_space=pltpu.HBM)
    bf = jnp.bfloat16
    return pl.pallas_call(
        functools.partial(layer_kernel, Z, Y, T, nk, paired),
        out_shape=(
            jax.ShapeDtypeStruct((rows * fs, g.shape[1]), bf),
            jax.ShapeDtypeStruct((rows * fs, g.shape[1]), bf),
            jax.ShapeDtypeStruct((rows_d * Y, d.shape[1] * T), bf),
            jax.ShapeDtypeStruct((n, d.shape[1]), bf),
        ),
        in_specs=[hbm] * 5,
        out_specs=[vmem] * 4,
        scratch_shapes=[
            pltpu.VMEM(gain.shape, jnp.float32),
            pltpu.VMEM(g.shape, jnp.float32), pltpu.VMEM(u.shape, jnp.float32), pltpu.VMEM(d.shape, jnp.float32),
            pltpu.VMEM(d.shape, bf), pltpu.VMEM(d.shape, bf), pltpu.VMEM(x.shape, bf), pltpu.VMEM((n, g.shape[1]), bf),
            pltpu.VMEM((n, nc * W), bf), pltpu.VMEM((n, nc * W), bf), pltpu.VMEM((n, nc * W), bf),
            pltpu.VMEM((max(X - 1, 1), n, pq * W), bf),
            dma((1,)), dma((nk,)), dma((nk,)), dma((1,)), dma((1,)),
            dma((1,)), dma((1,)), dma((lanes,)), dma((1,)), dma((Z, nk)), dma((fs,)),
            dma((1,)), dma((1,)), dma((1,)), dma((pq,)),
            dma((2,)), dma((lanes,)), dma((Y, nc)),
            dma((1,)), dma((nc // grain + 1,)), dma((1,)), dma((max(X - 1, 1), pq // grain)),
        ],
        compiler_params=pltpu.CompilerParams(
            collective_id=0, has_side_effects=True, vmem_limit_bytes=GRANT
        ),
        name="layer",
    )(*(pltpu.with_memory_space_constraint(v, pltpu.HBM) for v in (gain, g, u, d, x)))


def publish_kernel(cuts, wg, wu, wd, mixed, og, ou, od, om, sems):
    outs = []
    for a, (s, d) in enumerate(((wg, og), (wu, ou), (wd, od), (mixed, om))):
        h = s.shape[0] // cuts
        for i in range(cuts):
            outs.append(pltpu.make_async_copy(s.at[pl.ds(i * h, h), :], d.at[pl.ds(i * h, h), :], sems.at[a, i]))
    for c in outs:
        c.start()
    for c in outs:
        c.wait()


def publish(*arrays):
    vmem, any_ = pl.BlockSpec(memory_space=pltpu.VMEM), pl.BlockSpec(memory_space=pl.ANY)
    return pl.pallas_call(
        functools.partial(publish_kernel, CUTS),
        out_shape=tuple(jax.ShapeDtypeStruct(a.shape, a.dtype) for a in arrays),
        in_specs=[vmem] * 4,
        out_specs=[any_] * 4,
        scratch_shapes=[pltpu.SemaphoreType.DMA((4, CUTS))],
        compiler_params=pltpu.CompilerParams(vmem_limit_bytes=1024 * 1024),
        name="publish",
    )(*arrays)


def solution(mesh):
    def on_device(tokens, norm_gain, gate_weight, up_weight, down_weight):
        wg, wu, wd, mixed = layer(mesh, norm_gain[None, :], gate_weight, up_weight, down_weight, tokens)
        og, ou, od, om = publish(wg, wu, wd, mixed)
        return (om, og, ou, od)

    return jax.shard_map(
        on_device,
        mesh=mesh,
        in_specs=(P("fs", None), P("fs"), P("fs", "tp"), P("fs", "tp"), P("fs", "tp")),
        out_specs=(P("fs", "tp"), P(None, "tp"), P(None, "tp"), P("tp", None)),
        check_vma=False,
    )
```

```python
import functools

import jax
import jax.numpy as jnp
from jax import lax
from jax.experimental import pallas as pl
from jax.experimental.pallas import tpu as pltpu
from jax.sharding import PartitionSpec as P

MESH = pl.DeviceIdType.MESH
GRANT = 26 * 1024 * 1024
CUTS = 4
W = 128


def lines(fs):
    y = 1
    while 2 * (2 * y) * (2 * y) <= fs:
        y *= 2
    return fs // y, y


def when(cond, fn):
    pl.when(cond)(fn)


def each(lo, hi, fn):
    if hi > lo:
        pl.loop(lo, hi)(fn)


def layer_kernel(
    Z, Y, T, nk, paired,
    gain_hbm, g_hbm, u_hbm, d_hbm, x_hbm,
    wg, wu, wd, mixed,
    gain_row, stage_g, stage_u, stage_d, own_d, transit, normed, hidden, part, near, pair, far,
    in_gain, in_g, in_u, in_d, in_x, s_up, s_dn, s_y, s_det, r_w, r_o, s_one, s_tz, s_tx, r_t,
    s_dz, s_dy, r_d, s_a, r_a, s_b, r_b,
):
    f, t = lax.axis_index("fs"), lax.axis_index("tp")
    X = T // 2
    z, y = f // Y, lax.rem(f, Y)
    x, core = t // 2, lax.rem(t, 2)
    has_up, has_dn = z < Z - 1, z > 0
    up, dn = (f + Y, t), (f - Y, t)
    others = [lax.rem(y + i, Y) for i in range(1, Y)]
    across = [(z * Y + o, t) for o in others]
    rows = g_hbm.shape[0]
    ck = rows // nk
    rows_d, cols_d = d_hbm.shape
    pq = cols_d // W
    nc = T * pq
    n = x_hbm.shape[0]
    staged, full = (stage_g, stage_u), (wg, wu)
    pieces = [(k, a) for k in range(nk) for a in range(2)]

    def load(k, a):
        at = pl.ds(k * ck, ck)
        return pltpu.make_async_copy((g_hbm, u_hbm)[a].at[at, :], staged[a].at[at, :], (in_g, in_u)[a].at[k])

    load_d = pltpu.make_async_copy(d_hbm, stage_d, in_d.at[0])
    load_x = pltpu.make_async_copy(x_hbm, normed, in_x.at[0])
    load_gain = pltpu.make_async_copy(gain_hbm, gain_row, in_gain.at[0])
    load_gain.start()
    for k, a in pieces:
        load(k, a).start()
    load_d.start()
    load_x.start()

    barrier = pltpu.get_barrier_semaphore()

    def greet(dev):
        pl.semaphore_signal(barrier, inc=1, device_id=dev, device_id_type=MESH)

    when(has_up, lambda: greet(up))
    when(has_dn, lambda: greet(dn))
    for dev in across:
        greet(dev)
    for i in range(1, T):
        greet((f, lax.rem(t + i, T)))

    load_gain.wait()
    diagonal = lax.broadcasted_iota(jnp.int32, (rows, rows), 0) == lax.broadcasted_iota(jnp.int32, (rows, rows), 1)
    gain = jnp.sum(jnp.where(diagonal, jnp.broadcast_to(gain_row[...], (rows, rows)), 0.0), axis=1, keepdims=True)

    def copy(src, dst, ss, rs, dev):
        return pltpu.make_async_remote_copy(
            src_ref=src, dst_ref=dst, send_sem=ss, recv_sem=rs, device_id=dev, device_id_type=MESH
        )

    def weight(a, k, source, ss, rs, dev):
        at = full[a].at[pl.ds(pl.multiple_of(source * rows + k * ck, ck), ck), :]
        return copy(at, at, ss, rs, dev)

    def along(a, k, source, ss, dev):
        return weight(a, k, source, ss, r_w.at[source // Y, k], dev)

    def beyond_line(a, k, source, ss, dev):
        return weight(a, k, source, ss, r_o.at[source], dev)

    def taken(height, ss, rs):
        at = wg.at[pl.ds(0, height), :]
        return copy(at, at, ss, rs, (f, lax.rem(t + 1, T)))

    def arrived(k, source):
        taken(2 * ck, s_det.at[0], r_w.at[source // Y, k]).wait_recv()

    def arrived_whole(source):
        taken(2 * rows, s_det.at[0], r_o.at[source]).wait_recv()

    def start(cond, make):
        if cond is None:
            make().start()
        else:
            when(cond, lambda: make().start())

    def scale(k, a):
        load(k, a).wait()
        at = pl.ds(pl.multiple_of(f * rows + k * ck, ck), ck)
        full[a][at, :] = (gain[k * ck:(k + 1) * ck, :] * staged[a][pl.ds(k * ck, ck), :]).astype(jnp.bfloat16)

    def send_own(k, a):
        start(has_up, lambda: along(a, k, f, s_up.at[0], up))
        start(has_dn, lambda: along(a, k, f, s_dn.at[0], dn))
        for i in range(Y - 1):
            start(None, lambda i=i: beyond_line(a, k, f, s_y.at[i], across[i]))

    scale(*pieces[0])
    scale(*pieces[1])
    pl.semaphore_wait(barrier, Y + T - 2 + has_up.astype(jnp.int32) + has_dn.astype(jnp.int32))
    for i, piece in enumerate(pieces):
        if i + 2 < len(pieces):
            scale(*pieces[i + 2])
        send_own(*piece)

    def cols(j):
        return pl.ds(pl.multiple_of(j * W, W), W)

    def line_rows(line):
        return pl.ds(pl.multiple_of(line * rows_d, rows_d), rows_d)

    def down(line, j, ss, dev):
        at = wd.at[line_rows(line), cols(j)]
        return copy(at, at, ss, r_d.at[line, j], dev)

    def down_arrived(line, j):
        down(line, j, s_dy.at[0], (f, lax.rem(t + 1, T))).wait_recv()

    load_d.wait()
    own_d[...] = stage_d[...].astype(jnp.bfloat16)

    @pl.when(z == t)
    def _():
        wd[line_rows(y), pl.ds(pl.multiple_of(t * cols_d, cols_d), cols_d)] = stage_d[...].astype(jnp.bfloat16)

    def first(p):
        return copy(
            own_d.at[:, pl.ds(p * W, W)], wd.at[line_rows(y), cols(t * pq + p)],
            s_one.at[0], r_d.at[y, t * pq + p], (f, z),
        )

    load_x.wait()
    slab = 64 if n % 64 == 0 else n

    def normalise(i):
        at = pl.ds(pl.multiple_of(i * slab, slab), slab)
        v = normed[at, :].astype(jnp.float32)
        normed[at, :] = (v * lax.rsqrt(jnp.mean(v * v, axis=1, keepdims=True) + 1e-05)).astype(jnp.bfloat16)

    normalise(0)
    for p in range(pq):
        start(z != t, lambda p=p: first(p))
    each(1, n // slab, normalise)

    at_home = z == t
    can_up = jnp.logical_and(has_up, z >= t)
    can_dn = jnp.logical_and(has_dn, z <= t)
    inner = jnp.logical_and(has_up, has_dn)
    if paired:
        half = t // (T // 2)
        shift = (nc // 2) * (1 - half)
        far_up, far_dn = half == 0, half == 1
        beyond = jnp.logical_or(jnp.logical_and(z < t, far_dn), jnp.logical_and(z > t, far_up))
        fwd_mid = jnp.logical_or(
            jnp.logical_and(can_up, jnp.logical_not(far_up)), jnp.logical_and(can_dn, jnp.logical_not(far_dn))
        )
    fwd_all = jnp.logical_or(can_up, can_dn)
    if paired:
        passes = jnp.logical_or(fwd_all, beyond)
    away = jnp.logical_not(at_home)

    def column(r):
        return lax.rem(r + shift, nc)

    if paired:
        bent = (pq, lambda i: column(core * pq + i))
        low = (pq, lambda i: column((1 - core) * pq + i))
        mid = (pq // 2, lambda i: column((2 + core) * pq + i))
        high = (
            (pq, lambda i: column((3 - core) * pq + i)),
            (pq // 2, lambda i: column((2 + core) * pq + pq // 2 + i)),
        )
    else:
        mid = (nc, lambda i: i)
        high = ()
    high_count = sum(kind[0] for kind in high)

    def over(kind, fn):
        each(0, kind[0], lambda i: fn(kind[1](i)))

    def both(a, b):
        return jnp.logical_and(a, b)

    def kinds(j):
        r = lax.rem(j - shift + nc, nc)
        quarter = r // pq
        is_bent = quarter == core
        is_mid = jnp.logical_or(quarter == 1 - core, both(quarter == 2 + core, lax.rem(r, pq) < pq // 2))
        return jnp.logical_not(jnp.logical_or(is_bent, is_mid)), is_bent, is_mid

    def z_send(line, j, direction):
        return down(line, j, s_dz.at[direction], (up, dn)[direction])

    def near_ok(direction):
        return jnp.logical_not((far_up, far_dn)[direction])

    def can(direction):
        return (can_up, can_dn)[direction]

    def cross(j):
        for i in range(Y - 1):
            down(y, j, s_dy.at[i], across[i]).start()

    other = others[0]

    def assemble():
        for i in range(1, T):
            owner = lax.rem(t + i, T)
            for p in range(pq):
                down_arrived(y, owner * pq + p)
        for kind in high:
            over(kind, cross)
        if paired:
            @pl.when(inner)
            def _():
                over(low, cross)
                over(mid, cross)

    if paired:
        guest = lax.rem(t + T // 2, T)
        guest_dn = guest // (T // 2) == 1
        guest_here = jnp.logical_or(both(z < guest, guest_dn), both(z > guest, jnp.logical_not(guest_dn)))
        guest_on = (both(both(z >= guest, has_up), jnp.logical_not(guest_dn)), both(both(z <= guest, has_dn), guest_dn))

        def relay(p, direction, src):
            return copy(
                src.at[:, cols(p)], transit.at[:, cols(p)], s_tz.at[0], r_t.at[p], (up, dn)[direction]
            )

        def hand_over(p):
            return copy(
                transit.at[:, cols(p)], wd.at[line_rows(y), cols(t * pq + p)], s_tx.at[0], r_d.at[y, t * pq + p], (f, guest)
            )

    def leave(direction):
        if paired:
            @pl.when(both(z == guest, guest_on[direction]))
            def _():
                each(0, pq, lambda p: relay(p, direction, own_d).start())

        here = both(at_home, can(direction))
        if paired:
            here = both(here, jnp.logical_not(near_ok(direction)))

        @pl.when(here)
        def _():
            for kind in ((low, mid) if paired else (mid,)) + high:
                over(kind, lambda j: z_send(y, j, direction).start())

    def hook(s):
        when(z == s, lambda: leave(0))
        when(z == Z - 1 - s, lambda: leave(1))

    for step in range(1, Z):
        for k in range(nk):
            if step == 1 and k == nk // 2:
                when(at_home, assemble)
            for sign in (-1, 1):
                zs = z + sign * step
                source = zs * Y + y
                valid = zs >= 0 if sign < 0 else zs < Z
                onward = jnp.logical_and(valid, has_up if sign < 0 else has_dn)
                crossing = valid
                if paired and step == 1:
                    crossing = both(valid, zs != (0 if sign < 0 else Z - 1))
                when(valid, lambda k=k, s=source: arrived(k, s))
                for a in range(2):
                    if sign < 0:
                        start(onward, lambda a=a, k=k, s=source: along(a, k, s, s_up.at[0], up))
                    else:
                        start(onward, lambda a=a, k=k, s=source: along(a, k, s, s_dn.at[0], dn))
                    for i in range(Y - 1):
                        start(crossing, lambda a=a, k=k, s=source, i=i: beyond_line(a, k, s, s_y.at[i], across[i]))
        if step == 1:
            hook(0)
            if paired:
                ends = jnp.logical_not(inner)
                beside = across[0][0]
                when(ends, lambda: arrived_whole(beside))
                for k, a in pieces:
                    start(both(ends, has_up), lambda a=a, k=k: beyond_line(a, k, beside, s_det.at[0], up))
                    start(both(ends, has_dn), lambda a=a, k=k: beyond_line(a, k, beside, s_det.at[0], dn))
        hook(step)

    if paired:
        @pl.when(at_home)
        def _():
            @pl.when(jnp.logical_not(inner))
            def _():
                for kind in (bent, low, mid):
                    over(kind, cross)
            when(inner, lambda: over(bent, cross))

    else:
        when(at_home, lambda: over(mid, cross))

    if paired:
        @pl.when(guest_here)
        def _():
            def pass_on(p):
                copy(
                    transit.at[:, cols(p)], transit.at[:, cols(p)], s_tz.at[0], r_t.at[p], (f, guest)
                ).wait_recv()
                for direction in range(2):
                    when(guest_on[direction], lambda: relay(p, direction, transit).start())
                hand_over(p).start()
            each(0, pq, pass_on)

    if paired:
        @pl.when(both(at_home, inner))
        def _():
            def near_first(j):
                for direction in range(2):
                    when(near_ok(direction), lambda: z_send(y, j, direction).start())
            over(bent, near_first)

            def near_pair(is_high):
                def fn(j):
                    near_first(j)
                    down_arrived(other, j)
                    for direction in range(2):
                        toward = can(direction) if is_high else near_ok(direction)
                        when(toward, lambda: z_send(other, j, direction).start())
                return fn

            over(low, near_pair(False))
            for kind in high:
                over(kind, near_pair(True))
            over(mid, near_pair(False))

    @pl.when(away)
    def _():
        def bend(j):
            down_arrived(y, j)
            for direction in range(2):
                when(both(can(direction), near_ok(direction)), lambda: z_send(y, j, direction).start())
            cross(j)

        def straight(j):
            down_arrived(y, j)
            for direction in range(2):
                when(can(direction), lambda: z_send(y, j, direction).start())
            if paired:
                when(beyond, lambda: cross(j))
            else:
                cross(j)

        if paired:
            when(passes, lambda: over(low, straight))
            over(bent, bend)
            when(passes, lambda: over(mid, straight))
        else:
            over(mid, straight)

    if paired:
        @pl.when(both(fwd_mid, away))
        def _():
            def twin(j):
                down_arrived(other, j)
                for direction in range(2):
                    when(both(can(direction), near_ok(direction)), lambda: z_send(other, j, direction).start())
            over(low, twin)
            over(mid, twin)

        @pl.when(both(fwd_all, jnp.logical_or(away, jnp.logical_not(inner))))
        def _():
            def twins(j):
                @pl.when(away)
                def _():
                    down_arrived(y, j)
                    for direction in range(2):
                        when(can(direction), lambda: z_send(y, j, direction).start())
                down_arrived(other, j)
                for direction in range(2):
                    when(can(direction), lambda: z_send(other, j, direction).start())
            for kind in high:
                over(kind, twins)

    for zs in range(Z):
        for o in others:
            if paired and zs in (0, Z - 1):
                when(zs != z, lambda zs=zs, o=o: arrived_whole(zs * Y + o))
            else:
                arrived_whole(zs * Y + o)
    units = wg.shape[1]
    width = 256 if units % 256 == 0 else 128

    @pl.loop(0, units // width)
    def _(j):
        at = pl.ds(pl.multiple_of(j * width, width), width)
        gate = jnp.dot(normed[...], wg[:, at], preferred_element_type=jnp.float32)
        up_ = jnp.dot(normed[...], wu[:, at], preferred_element_type=jnp.float32)
        hidden[:, at] = (gate / (1.0 + jnp.exp(-gate)) * up_).astype(jnp.bfloat16)

    def drained(cond, shards, sem):
        when(cond, lambda: taken(2 * rows * shards, sem, r_w.at[0, 0]).wait_send())

    for q in range(Z - 1):
        drained(z == q, q + 1, s_up.at[0])
        drained(z == Z - 1 - q, q + 1, s_dn.at[0])
    for i in range(Y - 1):
        if paired:
            drained(inner, Z - 1, s_y.at[i])
            drained(jnp.logical_not(inner), Z, s_y.at[i])
        else:
            drained(z >= 0, Z, s_y.at[i])
    if paired:
        drained(jnp.logical_not(inner), 1, s_det.at[0])

    mate = (f, x * 2 + 1 - core)

    def span(j, count):
        return pl.ds(pl.multiple_of(j * W, W), count * W)

    grain = 2 if pq % 2 == 0 else 1

    def to_mate(j, count):
        at, lone = span(j, count), j // grain
        if count < grain:
            odd = lax.rem(j, grain)
            lone = odd * (nc // grain) + (1 - odd) * lone
        return copy(part.at[:, at], near.at[:, at], s_a.at[0], r_a.at[lone], mate)

    def to_owner(j, count, slot, dev):
        p = lax.rem(j, pq)
        return copy(
            pair.at[:, span(j, count)], far.at[slot, :, span(p, count)], s_b.at[0], r_b.at[slot, p // grain], dev
        )

    def whole(j):
        if paired:
            is_high, is_bent, is_mid = kinds(j)
            late = both(is_high, jnp.logical_not(fwd_all))
            late_own = both(away, jnp.logical_or(late, both(is_mid, jnp.logical_not(passes))))
            when(late_own, lambda: down_arrived(y, j))
            late_other = jnp.logical_or(jnp.logical_or(late, is_bent), both(is_mid, jnp.logical_not(fwd_mid)))
            when(late_other, lambda: down_arrived(other, j))
        else:
            for o in others:
                down_arrived(o, j)

    def ours(j):
        return lax.rem(j // pq, 2) == core

    def multiply(j, count):
        for i in range(count):
            whole(j + i)
        at = span(j, count)
        part[:, at] = jnp.dot(hidden[...], wd[:, at], preferred_element_type=jnp.float32).astype(jnp.bfloat16)
        when(jnp.logical_not(ours(j)), lambda: to_mate(j, count).start())

    def pass_sum(j, count):
        owner, at = j // pq, span(j, count)
        to_mate(j, count).wait_recv()
        pair[:, at] = (part[:, at].astype(jnp.float32) + near[:, at].astype(jnp.float32)).astype(jnp.bfloat16)
        to_owner(j, count, lax.rem(x - owner // 2 + X, X) - 1, (f, owner)).start()

    def sums_arrived(j):
        to_mate(j, grain).wait_recv()
        for slot in range(X - 1):
            to_owner(j, grain, slot, mate).wait_recv()

    def finish(j, count):
        at, to = span(j, count), span(lax.rem(j, pq), count)
        acc = part[:, at].astype(jnp.float32) + near[:, at].astype(jnp.float32)
        for slot in range(X - 1):
            acc = acc + far[slot, :, to].astype(jnp.float32)
        mixed[:, to] = acc.astype(mixed.dtype)

    if paired:
        upper = (z >= Z // 2).astype(jnp.int32)
        is_far = half == 1 - upper
        is_edge = jnp.logical_or(t == 0, t == T - 1)
        block_a, block_b, block_c, block_d = core * pq, (1 - core) * pq, (2 + core) * pq, (3 - core) * pq
        orders = (
            (block_b, block_d, block_b + 2, block_a, block_d + 2, block_a + 2,
             block_c + 2, block_c, block_c + 3, block_c + 1),
            (block_c, block_c + 2, block_b, block_b + 2, block_a + 2, block_d,
             block_d + 2, block_d + 3, block_a, block_a + 1),
            (block_c, block_d, block_d + 2, block_c + 2, block_b, block_b + 2,
             block_a + 2, block_a + 3, block_a, block_a + 1),
        )
        turn = upper * (nc // 2)
        chosen = [
            lax.rem(jnp.where(is_far, v, jnp.where(is_edge, e, i)) + turn, nc) for v, e, i in zip(*orders)
        ]
        doubles, singles = chosen[:6], chosen[6:]

        def pick(table, i):
            return sum(v * (i == e).astype(jnp.int32) for e, v in enumerate(table))

        over_there = lax.rem(t + T // 2, T) * pq
        first_at = jnp.where(is_far, 3, jnp.where(is_edge, 0, 5))
        second_at = jnp.where(is_far, 5, jnp.where(is_edge, 1, 6))

        def double(i):
            multiply(pick(doubles, i), grain)
            second = i == second_at
            when(jnp.logical_or(i == first_at, second), lambda: pass_sum(over_there + second.astype(jnp.int32) * grain, grain))

        def single(i):
            multiply(pick(singles, i), 1)
            when(both(i < grain, second_at == 6), lambda: pass_sum(over_there + grain + i, 1))

        each(0, len(doubles), double)
        each(0, len(singles), lambda i: when(jnp.logical_or(i < len(singles) - 1, is_far), lambda: single(i)))
        each(0, pq // grain, lambda i: sums_arrived(t * pq + i * grain))
        finish(t * pq + 2, 2)
        finish(t * pq, 1)
        when(jnp.logical_not(is_far), lambda: multiply(singles[-1], 1))
        finish(t * pq + 1, 1)
    else:
        each(0, nc // grain, lambda i: multiply(i * grain, grain))
        for i in range(1, X):
            base = (lax.rem(x + i, X) * 2 + core) * pq
            each(0, pq // grain, lambda i, base=base: pass_sum(base + i * grain, grain))
        each(0, pq // grain, lambda i: sums_arrived(t * pq + i * grain))
        each(0, pq // grain, lambda i: finish(t * pq + i * grain, grain))

    def gone(sem, ref):
        copy(ref, ref, sem, r_a.at[0], mate).wait_send()

    def gone_down(cond, sem, count):
        fold = next(c for c in range(1, Y + 1) if count % c == 0 and count // c <= nc)
        when(cond, lambda: gone(sem, wd.at[pl.ds(0, fold * rows_d), pl.ds(0, count // fold * W)]))

    when(away, lambda: gone(s_one.at[0], own_d))
    if paired:
        when(jnp.logical_or(guest_on[0], guest_on[1]), lambda: gone(s_tz.at[0], transit))
        when(guest_here, lambda: gone(s_tx.at[0], transit))
        for direction in range(2):
            gone_down(both(can(direction), near_ok(direction)), s_dz.at[direction], 2 * nc - pq)
            on = both(can(direction), jnp.logical_not(near_ok(direction)))
            gone_down(on, s_dz.at[direction], nc - pq + high_count)
        gone_down(at_home, s_dy.at[0], nc)
        gone_down(beyond, s_dy.at[0], nc - high_count)
        gone_down(both(away, jnp.logical_not(beyond)), s_dy.at[0], pq)
    else:
        for direction in range(2):
            gone_down(can(direction), s_dz.at[direction], nc)
        for i in range(Y - 1):
            gone_down(z >= 0, s_dy.at[i], nc)
    gone(s_a.at[0], part.at[:, pl.ds(0, nc * W // 2)])
    gone(s_b.at[0], pair.at[:, pl.ds(0, (X - 1) * pq * W)])


def layer(mesh, gain, g, u, d, x):
    fs, T = mesh.shape["fs"], mesh.shape["tp"]
    Z, Y = lines(fs)
    X = T // 2
    rows, rows_d, n = g.shape[0], d.shape[0], x.shape[0]
    pq = d.shape[1] // W
    nc = T * pq
    nk = max(1, min(4, rows // 64))
    paired = Y == 2 and X == 2 and Z == T and pq == 4
    grain = 2 if pq % 2 == 0 else 1
    lanes = max(Y - 1, 1)
    dma = pltpu.SemaphoreType.DMA
    vmem, hbm = pl.BlockSpec(memory_space=pltpu.VMEM), pl.BlockSpec(memory_space=pltpu.HBM)
    bf = jnp.bfloat16
    return pl.pallas_call(
        functools.partial(layer_kernel, Z, Y, T, nk, paired),
        out_shape=(
            jax.ShapeDtypeStruct((rows * fs, g.shape[1]), bf),
            jax.ShapeDtypeStruct((rows * fs, g.shape[1]), bf),
            jax.ShapeDtypeStruct((rows_d * Y, d.shape[1] * T), bf),
            jax.ShapeDtypeStruct((n, d.shape[1]), bf),
        ),
        in_specs=[hbm] * 5,
        out_specs=[vmem] * 4,
        scratch_shapes=[
            pltpu.VMEM(gain.shape, jnp.float32),
            pltpu.VMEM(g.shape, jnp.float32), pltpu.VMEM(u.shape, jnp.float32), pltpu.VMEM(d.shape, jnp.float32),
            pltpu.VMEM(d.shape, bf), pltpu.VMEM(d.shape, bf), pltpu.VMEM(x.shape, bf), pltpu.VMEM((n, g.shape[1]), bf),
            pltpu.VMEM((n, nc * W), bf), pltpu.VMEM((n, nc * W), bf), pltpu.VMEM((n, nc * W), bf),
            pltpu.VMEM((max(X - 1, 1), n, pq * W), bf),
            dma((1,)), dma((nk,)), dma((nk,)), dma((1,)), dma((1,)),
            dma((1,)), dma((1,)), dma((lanes,)), dma((1,)), dma((Z, nk)), dma((fs,)),
            dma((1,)), dma((1,)), dma((1,)), dma((pq,)),
            dma((2,)), dma((lanes,)), dma((Y, nc)),
            dma((1,)), dma((nc // grain + 1,)), dma((1,)), dma((max(X - 1, 1), pq // grain)),
        ],
        compiler_params=pltpu.CompilerParams(
            collective_id=0, has_side_effects=True, vmem_limit_bytes=GRANT
        ),
        name="layer",
    )(*(pltpu.with_memory_space_constraint(v, pltpu.HBM) for v in (gain, g, u, d, x)))


def publish_kernel(cuts, wg, wu, wd, mixed, og, ou, od, om, sems):
    outs = []
    for a, (s, d) in enumerate(((wg, og), (wu, ou), (wd, od), (mixed, om))):
        h = s.shape[0] // cuts
        for i in range(cuts):
            outs.append(pltpu.make_async_copy(s.at[pl.ds(i * h, h), :], d.at[pl.ds(i * h, h), :], sems.at[a, i]))
    for c in outs:
        c.start()
    for c in outs:
        c.wait()


def publish(*arrays):
    vmem, any_ = pl.BlockSpec(memory_space=pltpu.VMEM), pl.BlockSpec(memory_space=pl.ANY)
    return pl.pallas_call(
        functools.partial(publish_kernel, CUTS),
        out_shape=tuple(jax.ShapeDtypeStruct(a.shape, a.dtype) for a in arrays),
        in_specs=[vmem] * 4,
        out_specs=[any_] * 4,
        scratch_shapes=[pltpu.SemaphoreType.DMA((4, CUTS))],
        compiler_params=pltpu.CompilerParams(vmem_limit_bytes=1024 * 1024),
        name="publish",
    )(*arrays)


def solution(mesh):
    def on_device(tokens, norm_gain, gate_weight, up_weight, down_weight):
        wg, wu, wd, mixed = layer(mesh, norm_gain[None, :], gate_weight, up_weight, down_weight, tokens)
        og, ou, od, om = publish(wg, wu, wd, mixed)
        return (om, og, ou, od)

    return jax.shard_map(
        on_device,
        mesh=mesh,
        in_specs=(P("fs", None), P("fs"), P("fs", "tp"), P("fs", "tp"), P("fs", "tp")),
        out_specs=(P("fs", "tp"), P(None, "tp"), P(None, "tp"), P("tp", None)),
        check_vma=False,
    )
```
